32 devices in a mesh: sp: 8 (over z, y), tp: 4 (over x, core).
Axes of the slice: x: 2, y: 2, z: 4, core: 2. Of those that a mesh axis runs over, the one named last changes fastest.
Arguments:
- tokens: bfloat16 [2048, 2048], P('sp', 'tp'), may hold values from -19 to 250
- in_gain: bfloat16 [2048], replicated, may hold values from 0.099609375 to 1.8984375
- w_glu_value: bfloat16 [2048, 512], P(None, 'tp'), may hold values from -0.125 to 0.125
- w_glu_gate: bfloat16 [2048, 512], P(None, 'tp'), may hold values from -0.125 to 0.125
- w_query: bfloat16 [2048, 1024], P(None, 'tp'), may hold values from -1 to 1
- w_key: bfloat16 [2048, 512], P(None, 'tp'), may hold values from -1 to 1
- w_value: bfloat16 [2048, 512], P(None, 'tp'), may hold values from -0.125 to 0.125
- w_gate_conv: bfloat16 [2048, 512], P(None, 'tp'), may hold values from -0.125 to 0.125
- w_gate_attn: bfloat16 [2048, 1024], P(None, 'tp'), may hold values from -0.125 to 0.125
- conv_weight: bfloat16 [31, 512], P(None, 'tp'), may hold values from -4.6 to 4.6
- conv_gain: float32 [512], P('tp'), may hold values from 0.1 to 1.9
- lam: float32 [8], P('tp'), may hold values from 0.3 to 0.8
- head_gain: float32 [128], replicated, may hold values from 0.1 to 1.9
- out_conv: bfloat16 [512, 2048], P('tp'), may hold values from -0.15625 to 0.15625
- out_attn: bfloat16 [1024, 2048], P('tp'), may hold values from -0.15625 to 0.15625
Outputs:
- mixed: bfloat16 [2048, 2048], P(('sp', 'tp'))
The draws below stay inside these ranges and needn't reach their ends.
All inputs are finite; a program needn't handle non-finite values.
Results may differ from the reference program's by a relative error of at most 0.017.
The reference program's roundings to bfloat16 on the way count: a program that leaves them out, or rounds other values in their place, can miss the bound.
Values may be sent and summed in bfloat16 or wider, within the bound.
A program may use at most 128 MiB of HBM per device.

```python
import math
import jax
import jax.numpy as jnp
from jax import lax

D = 2048
CONV = 512
HEADS = 8
KV_HEADS = 4
QK = 64
VDIM = 128
WIDTH = 31
TOKENS = 2048
N_TP = 4


def draw_tokens(key, part):
    k_base = jax.random.fold_in(jax.random.fold_in(key, 11), 0)
    values = jnp.clip(jax.random.normal(k_base, (TOKENS, D), jnp.float32), -6.0, 6.0)
    return values.astype(jnp.bfloat16)


def draw_w_query(key, part):
    values = jnp.clip(jax.random.normal(jax.random.fold_in(key, 21), (D, HEADS * 2 * QK), jnp.float32), -6.0, 6.0)
    values = values * (1.3 / jnp.sqrt(jnp.float32(D)))
    return values.astype(jnp.bfloat16)


def draw_w_key(key, part):
    values = jnp.clip(jax.random.normal(jax.random.fold_in(key, 22), (D, KV_HEADS * 2 * QK), jnp.float32), -6.0, 6.0)
    values = values * (1.3 / jnp.sqrt(jnp.float32(D)))
    return values.astype(jnp.bfloat16)


def draw_conv_weight(key, part):
    k_base, k_rough = jax.random.split(jax.random.fold_in(key, 31), 2)
    position = jnp.arange(CONV, dtype=jnp.float32) / CONV
    trend = 3.0 ** (position - 0.5)
    rough = jnp.exp(jax.random.uniform(k_rough, (CONV,), jnp.float32, -0.7, 0.7))
    values = jnp.clip(jax.random.normal(k_base, (WIDTH, CONV), jnp.float32), -4.0, 4.0)
    values = values / jnp.sqrt(jnp.float32(WIDTH)) * (trend * rough)[None, :]
    return values.astype(jnp.bfloat16)


def shard_levels(stream_key, shape, cuts, smallest, largest):
    gain, own = 1.0, jax.random.fold_in(stream_key, 6)
    for dim, parts in cuts:
        heights = jnp.exp(jax.random.uniform(jax.random.fold_in(own, dim), (parts,), jnp.float32, smallest / len(cuts), largest / len(cuts)))
        gain = gain * jnp.repeat(heights, shape[dim] // parts).reshape([-1 if axis == dim else 1 for axis in range(len(shape))])
    return gain


def gaussian(rng, shape, deviation, reach, cuts=(), kind=jnp.bfloat16):
    level = shard_levels(rng, shape, cuts, -0.22, 0.18) if cuts else 1.0
    entries = jax.random.normal(rng, shape, jnp.float32) * deviation * level
    return jnp.minimum(jnp.maximum(entries, -reach), reach).astype(kind)


def setup_inputs(seed: int = 0) -> dict:
    streams_of = jax.random.split(jax.random.key(seed), 16)
    return {
        "tokens": draw_tokens(jax.random.fold_in(streams_of[15], 71), 0),
        "in_gain": jnp.clip(1.0 + 0.18 * jax.random.normal(streams_of[1], (D,), jnp.float32), 0.099609375, 1.8984375).astype(jnp.bfloat16),
        "w_glu_value": gaussian(streams_of[2], (D, CONV), D ** -0.5, 0.125, ((1, 4),)),
        "w_glu_gate": gaussian(streams_of[3], (D, CONV), D ** -0.5, 0.125, ((1, 4),)),
        "w_query": draw_w_query(jax.random.fold_in(streams_of[15], 71), 0),
        "w_key": draw_w_key(jax.random.fold_in(streams_of[15], 71), 0),
        "w_value": gaussian(streams_of[6], (D, KV_HEADS * VDIM), D ** -0.5, 0.125, ((1, 4),)),
        "w_gate_conv": gaussian(streams_of[7], (D, CONV), D ** -0.5, 0.125, ((1, 4),)),
        "w_gate_attn": gaussian(streams_of[8], (D, HEADS * VDIM), D ** -0.5, 0.125, ((1, 4),)),
        "conv_weight": draw_conv_weight(jax.random.fold_in(streams_of[15], 71), 0),
        "conv_gain": jnp.clip(1.0 + 0.18 * jax.random.normal(streams_of[10], (CONV,), jnp.float32), 0.1, 1.9),
        "lam": jnp.clip(0.3 + 0.5 * jax.random.uniform(streams_of[11], (HEADS,), jnp.float32) ** shard_levels(streams_of[11], (HEADS,), ((0, 4),), -0.2, 0.2), 0.3, 0.8),
        "head_gain": jnp.clip(1.0 + 0.18 * jax.random.normal(streams_of[12], (VDIM,), jnp.float32), 0.1, 1.9),
        "out_conv": gaussian(streams_of[13], (CONV, D), (CONV + HEADS * VDIM) ** -0.5, 0.15625, ((0, 4),)),
        "out_attn": gaussian(streams_of[14], (HEADS * VDIM, D), (CONV + HEADS * VDIM) ** -0.5, 0.15625, ((0, 4),)),
    }


EPSILON = 1e-06
NEG_BIG = -1e+30
HEAD_SCALE = 0.8

def attend_head(query_head, key_head, value_head, lam_head, head_gain):
    block_rows = math.gcd(TOKENS, 512)
    blocks = TOKENS // block_rows
    scale_factor = 1.0 / math.sqrt(QK)

    def one_block(index):
        query_block = lax.dynamic_slice_in_dim(query_head, index * block_rows, block_rows, 0).astype(jnp.float32)
        query_pos = index * block_rows + jnp.arange(block_rows, dtype=jnp.int32)

        def visit(other, running):
            maxima, totals, summed = running
            key_block = lax.dynamic_slice_in_dim(key_head, other * block_rows, block_rows, 0).astype(jnp.float32)
            value_block = lax.dynamic_slice_in_dim(value_head, other * block_rows, block_rows, 0).astype(jnp.float32)
            scores = jnp.einsum('qcd,kcd->cqk', query_block, key_block) * scale_factor
            key_pos = other * block_rows + jnp.arange(block_rows, dtype=jnp.int32)
            scores = jnp.where(key_pos[None, None, :] <= query_pos[None, :, None], scores, NEG_BIG)
            new_max = jnp.maximum(maxima, lax.optimization_barrier(jnp.max(scores, axis=2)))
            factor = jnp.exp(maxima - new_max)
            expd = jnp.exp(scores - new_max[:, :, None])
            totals = totals * factor + lax.optimization_barrier(jnp.sum(expd, axis=2))
            rounded = lax.optimization_barrier(expd.astype(jnp.bfloat16)).astype(jnp.float32)
            summed = summed * factor[:, :, None] + jnp.einsum('cqk,kv->cqv', rounded, value_block)
            return (new_max, totals, summed)
        start_state = (jnp.full((2, block_rows), NEG_BIG, jnp.float32), jnp.zeros((2, block_rows), jnp.float32), jnp.zeros((2, block_rows, VDIM), jnp.float32))
        maxima, totals, summed = lax.fori_loop(0, index + 1, visit, start_state)
        output = summed[0] / totals[0][:, None] - lam_head * summed[1] / totals[1][:, None]
        normed = output * lax.rsqrt(lax.optimization_barrier(jnp.mean(output * output, axis=1, keepdims=True)) + EPSILON)
        return normed * head_gain[None, :] * HEAD_SCALE
    result = lax.map(one_block, jnp.arange(blocks, dtype=jnp.int32))
    return result.reshape(TOKENS, VDIM)

def reference(tokens, in_gain, w_glu_value, w_glu_gate, w_query, w_key, w_value, w_gate_conv, w_gate_attn, conv_weight, conv_gain, lam, head_gain, out_conv, out_attn):
    widened = tokens.astype(jnp.float32)
    inv_rms = lax.rsqrt(lax.optimization_barrier(jnp.mean(widened * widened, axis=1, keepdims=True)) + EPSILON)
    scaled = (widened * in_gain.astype(jnp.float32)[None, :]).astype(jnp.bfloat16)

    def project(weight):
        return (jnp.dot(scaled, weight, preferred_element_type=jnp.float32) * inv_rms).astype(jnp.bfloat16)
    glu_value = project(w_glu_value)
    glu_gate = project(w_glu_gate)
    query = project(w_query)
    key = project(w_key)
    value = project(w_value)
    gate_conv = project(w_gate_conv)
    gate_attn = project(w_gate_attn)
    glued = (glu_value.astype(jnp.float32) * jax.nn.sigmoid(glu_gate.astype(jnp.float32))).astype(jnp.bfloat16)
    padded = jnp.pad(glued.astype(jnp.float32), ((WIDTH - 1, 0), (0, 0)))
    taps = conv_weight.astype(jnp.float32)
    conv = jnp.zeros((TOKENS, CONV), jnp.float32)
    for offset in range(WIDTH):
        conv = conv + padded[offset:offset + TOKENS] * taps[offset][None, :]
    channel_ms = lax.optimization_barrier(jnp.mean(conv * conv, axis=1, keepdims=True))
    conv_normed = conv * lax.rsqrt(channel_ms + EPSILON) * conv_gain[None, :]
    y_conv = (jax.nn.silu(conv_normed) * jax.nn.silu(gate_conv.astype(jnp.float32))).astype(jnp.bfloat16)
    group = HEADS // KV_HEADS
    query_heads = jnp.transpose(query.reshape(TOKENS, HEADS, 2, QK), (1, 0, 2, 3))
    key_heads = jnp.transpose(key.reshape(TOKENS, KV_HEADS, 2, QK), (1, 0, 2, 3))
    value_heads = jnp.transpose(value.reshape(TOKENS, KV_HEADS, VDIM), (1, 0, 2))

    def per_head(head):
        shared = head // group
        return attend_head(query_heads[head], key_heads[shared], value_heads[shared], lam[head], head_gain)
    heads_out = lax.map(per_head, jnp.arange(HEADS, dtype=jnp.int32))
    attn_normed = jnp.transpose(heads_out, (1, 0, 2)).reshape(TOKENS, HEADS * VDIM)
    y_attn = (attn_normed * jax.nn.silu(gate_attn.astype(jnp.float32))).astype(jnp.bfloat16)
    conv_block = CONV // N_TP
    attn_block = HEADS * VDIM // N_TP
    mixed = jnp.zeros((TOKENS, D), jnp.float32)
    for member in range(N_TP):
        partial_value = jnp.dot(y_conv[:, member * conv_block:(member + 1) * conv_block], out_conv[member * conv_block:(member + 1) * conv_block], preferred_element_type=jnp.float32)
        partial_value = partial_value + jnp.dot(y_attn[:, member * attn_block:(member + 1) * attn_block], out_attn[member * attn_block:(member + 1) * attn_block], preferred_element_type=jnp.float32)
        mixed = mixed + lax.optimization_barrier(partial_value.astype(jnp.bfloat16)).astype(jnp.float32)
    return mixed.astype(jnp.bfloat16)
```

```python
import functools
import math

import jax
import jax.numpy as jnp
from jax import lax
from jax.experimental import pallas as pl
from jax.experimental.pallas import tpu as pltpu
from jax.sharding import PartitionSpec as P

EPSILON = 1e-06
NEG_BIG = -1e30
HEAD_SCALE = 0.8
QK = 64
VDIM = 128
MESH = pl.DeviceIdType.MESH
F32 = jnp.float32
BF16 = jnp.bfloat16
PIECES = 4
PAD = 32
LANES = 128
CHUNKS = 4
NEAR_STEPS = 3
SKIP = 3


def dot(a, b, ca=1, cb=0, precision=None):
    return lax.dot_general(
        a, b, (((ca,), (cb,)), ((), ())), preferred_element_type=F32, precision=precision
    )


def kernel(
    n_sp,
    n_tp,
    tok_hbm,
    gain_hbm,
    w_glu_value,
    w_glu_gate,
    w_query,
    w_key,
    w_value,
    w_gate_conv,
    w_gate_attn,
    taps_hbm,
    conv_gain_hbm,
    lam_hbm,
    head_gain_hbm,
    out_conv,
    out_attn,
    out,
    w_all,
    w_out,
    tokbuf,
    scaled_far,
    acc,
    kv,
    q4,
    m_ref,
    l_ref,
    o_ref,
    gl,
    tail_out,
    tail_in,
    sq_out,
    sq_in,
    ybuf,
    a_out,
    a_own,
    a_in,
    x_out,
    x_in,
    b_out,
    b_own,
    b_in,
    w_sem,
    tok_send,
    tok_recv,
    kv_recv,
    up_send,
    skip_send,
    side_send,
    tail_sem,
    sq_send,
    sq_recv,
    a_sem,
    x_sem,
    b_sem,
    gain32,
    tok,
    gain,
    taps_ref,
    conv_gain,
    lam,
    head_gain,
    ga,
    small_sem,
):
    rows, depth = tok.shape
    width = depth * n_tp
    s = lax.axis_index("sp")
    t = lax.axis_index("tp")
    core = t % 2
    p1 = t + 1 - 2 * core
    p2 = (t + 2) % n_tp
    p3 = (p1 + 2) % n_tp
    y = s % 2
    z = s // 2
    nz = n_sp // 2
    mate = s + 1 - 2 * y
    has_up = s + 2 < n_sp
    has_skip = s + 2 * SKIP < n_sp
    size = rows // CHUNKS
    last_static = min(NEAR_STEPS, nz - 1)

    smalls = [
        pltpu.make_async_copy(src, dst, small_sem.at[i])
        for i, (src, dst) in enumerate((
            (tok_hbm, tok), (gain_hbm, gain), (taps_hbm, taps_ref),
            (conv_gain_hbm, conv_gain), (lam_hbm, lam), (head_gain_hbm, head_gain),
        ))
    ]
    for copy in smalls:
        copy.start()
    weights = (w_key, w_value, w_glu_value, w_glu_gate, w_query, w_gate_conv, w_gate_attn)
    spans = []
    at = 0
    loads = []
    for i, w in enumerate(weights):
        cols = w.shape[1]
        spans.append((at, at + cols))
        loads.append(pltpu.make_async_copy(w, w_all.at[:, at : at + cols], w_sem.at[0]))
        at += cols
    at = 0
    out_loads = []
    for i, w in enumerate((out_conv, out_attn)):
        r = w.shape[0]
        out_loads.append(
            pltpu.make_async_copy(w, w_out.at[at : at + r, :], w_sem.at[1])
        )
        at += r

    def tp_copy(src, dst, send, recv, to):
        return pltpu.make_async_remote_copy(
            src_ref=src, dst_ref=dst, send_sem=send, recv_sem=recv,
            device_id={"tp": to}, device_id_type=MESH,
        )

    def sp_copy(src, dst, send, recv, to):
        return pltpu.make_async_remote_copy(
            src_ref=src, dst_ref=dst, send_sem=send, recv_sem=recv,
            device_id={"sp": to}, device_id_type=MESH,
        )

    barrier = pltpu.get_barrier_semaphore()
    for peer in (p1, p2, p3):
        pl.semaphore_signal(barrier, inc=1, device_id={"tp": peer}, device_id_type=MESH)
    expected = jnp.int32(3)
    for by in (1, 2, 2 * SKIP):
        for other in (s - by, s + by):
            valid = (other >= 0) & (other < n_sp)
            expected = expected + valid.astype(jnp.int32)

            @pl.when(valid)
            def _():
                pl.semaphore_signal(barrier, inc=1, device_id={"sp": other}, device_id_type=MESH)

    for copy in smalls:
        copy.wait()
    for copy in loads:
        copy.start()
    pl.semaphore_wait(barrier, expected)

    def piece_rows(q):
        return slice(q * size, (q + 1) * size)

    across = [
        tp_copy(
            tok.at[piece_rows(q)], tokbuf.at[1, piece_rows(q)],
            tok_send.at[0], tok_recv.at[q], p2,
        )
        for q in range(CHUNKS)
    ]
    passed = [
        tp_copy(
            tokbuf.at[1, piece_rows(q)], tokbuf.at[2, piece_rows(q)],
            tok_send.at[1], tok_recv.at[CHUNKS + q], p1,
        )
        for q in range(CHUNKS)
    ]
    beside = tp_copy(tok, tokbuf.at[0], tok_send.at[2], tok_recv.at[2 * CHUNKS], p1)
    for copy in across:
        copy.start()
    beside.start()
    for copy in out_loads:
        copy.start()

    lines = depth // LANES

    def prepare(x, owner):
        wide = x.astype(F32)
        parts = [
            wide[:, b * LANES : (b + 1) * LANES] * gain32[pl.ds(owner * lines + b, 1), :]
            for b in range(lines)
        ]
        scaled = jnp.concatenate(parts, axis=1).astype(BF16)
        return scaled, jnp.sum(wide * wide, axis=1, keepdims=True)

    def w_rows(owner, lo, hi):
        return w_all[pl.ds(pl.multiple_of(owner * depth, depth), depth), lo:hi]

    first_cols = spans[1][1]
    total_cols = spans[-1][1]
    gain32[...] = gain[...].astype(F32)
    scaled_own, squares = prepare(tok[...], t)
    pltpu.make_async_copy(w_all, w_all, w_sem.at[0]).wait()
    beside.wait_recv()
    scaled, more = prepare(tokbuf[0], p1)
    squares = squares + more
    acc[...] = dot(
        jnp.concatenate([scaled_own, scaled], axis=1),
        jnp.concatenate([w_rows(t, 0, total_cols), w_rows(p1, 0, total_cols)], axis=0),
    )

    def late(q):
        at = piece_rows(q)
        lhs = jnp.concatenate([scaled_far[0, at], scaled_far[1, at]], axis=1)
        rhs = jnp.concatenate(
            [w_rows(p2, first_cols, total_cols), w_rows(p3, first_cols, total_cols)], axis=0
        )
        acc[at, first_cols:] += dot(lhs, rhs)

    def chunk(j, q):
        return kv.at[j, :, piece_rows(q), :]

    def up(j, q):
        return sp_copy(chunk(j, q), chunk(j, q), up_send.at[j], kv_recv.at[j, q], s + 2)

    def skip(q):
        return sp_copy(chunk(s, q), chunk(s, q), skip_send.at[0], kv_recv.at[s, q], s + 2 * SKIP)

    def side(j, q):
        return sp_copy(chunk(j, q), chunk(j, q), side_send.at[j], kv_recv.at[j, q], mate)

    def relay(k, q):
        j = s - 2 * k
        up(j, q).wait_recv()
        if isinstance(k, int):
            if k != SKIP - 1:

                @pl.when(has_up)
                def _():
                    up(j, q).start()
        else:

            @pl.when(has_up & (k != SKIP - 1))
            def _():
                up(j, q).start()

        side(j, q).start()

    def due(k, q):
        lag = 2.4 * k if k < SKIP else 3.8
        return 6.9 + 1.4 * q + lag

    pending = sorted(
        ((k, q) for k in range(1, last_static + 1) for q in range(CHUNKS)),
        key=lambda e: due(*e),
    )

    def relays(until):
        while pending and due(*pending[0]) < until:
            k, q = pending.pop(0)

            @pl.when(z >= k)
            def _():
                relay(k, q)

    inv_parts = []
    for q in range(CHUNKS):
        at = piece_rows(q)
        across[q].wait_recv()
        passed[q].start()
        scaled, sq2 = prepare(tokbuf[1, at], p2)
        scaled_far[0, at] = scaled
        part = acc[at, :first_cols] + dot(scaled, w_rows(p2, 0, first_cols))
        if q > 0:
            late(q - 1)
        passed[q].wait_recv()
        scaled, sq3 = prepare(tokbuf[2, at], p3)
        scaled_far[1, at] = scaled
        part = part + dot(scaled, w_rows(p3, 0, first_cols))
        inv = lax.rsqrt((squares[at] + sq2 + sq3) / width + EPSILON)
        inv_parts.append(inv)
        part = (part * inv).astype(BF16)
        kv[s, 0, at] = part[:, : spans[0][1]]
        kv[s, 1, at] = part[:, spans[1][0] :]

        @pl.when(y == 0)
        def _():
            side(s, q).start()

        @pl.when(has_skip)
        def _():
            skip(q).start()

        @pl.when(has_up)
        def _():
            up(s, q).start()

        relays(7.2 + 1.3 * q)
    late(CHUNKS - 1)
    relays(11.8)
    inv_rms = jnp.concatenate(inv_parts, axis=0)

    def projected(i, lo=0, hi=None):
        hi = rows if hi is None else hi
        a, b = spans[i]
        return (acc[lo:hi, a:b] * inv_rms[lo:hi]).astype(BF16)

    def glue(lo, hi):
        value = projected(2, lo, hi).astype(F32)
        gate = projected(3, lo, hi).astype(F32)
        return (value * jax.nn.sigmoid(gate)).astype(BF16)

    tail_out[...] = glue(rows - PAD, rows)
    tail = sp_copy(tail_out, tail_in, tail_sem.at[0], tail_sem.at[1], s + 1)

    @pl.when(s + 1 < n_sp)
    def _():
        tail.start()

    query = projected(4).astype(F32) * (1.0 / math.sqrt(QK))
    heads = w_query.shape[1] // (2 * QK)
    maps = 2 * heads
    lane = lax.broadcasted_iota(jnp.int32, (rows, 2 * QK), 1)
    for h in range(heads):
        qh = query[:, h * 2 * QK : (h + 1) * 2 * QK]
        for m in range(2):
            keep = (lane >= m * QK) & (lane < (m + 1) * QK)
            q4[2 * h + m] = jnp.where(keep, qh, 0.0).astype(BF16)
    relays(12.6)

    key_pos = lax.broadcasted_iota(jnp.int32, (rows, rows), 0)
    query_pos = lax.broadcasted_iota(jnp.int32, (rows, rows), 1)
    allowed = key_pos <= query_pos
    k_own = kv[s, 0]
    v_own = kv[s, 1]
    scores = [jnp.where(allowed, dot(k_own, q4[i], 1, 1), NEG_BIG) for i in range(maps)]
    tops = [jnp.max(x, axis=0, keepdims=True) for x in scores]
    exps = [jnp.exp(x - top) for x, top in zip(scores, tops)]
    for i in range(maps):
        m_ref[i] = tops[i]
        l_ref[i] = jnp.sum(exps[i], axis=0, keepdims=True)
        o_ref[i] = dot(v_own, exps[i].astype(BF16), 0, 0)
    relays(13.6)

    gl[PAD:, :] = glue(0, rows).astype(F32)
    gate_attn = projected(6).astype(F32)
    ga[...] = gate_attn * jax.nn.sigmoid(gate_attn)

    def visit(blocks, at=slice(None)):
        def stacked(plane):
            parts = [kv[j, plane] for j in blocks]
            return parts[0] if len(parts) == 1 else jnp.concatenate(parts, axis=0)

        k = stacked(0)
        v = stacked(1)
        scores = [dot(k, q4[i, at, :], 1, 1) for i in range(maps)]
        olds = [m_ref[i, :, at] for i in range(maps)]
        tops = [
            jnp.maximum(old, jnp.max(x, axis=0, keepdims=True)) for old, x in zip(olds, scores)
        ]
        exps = [jnp.exp(x - top) for x, top in zip(scores, tops)]
        factors = [jnp.exp(old - top) for old, top in zip(olds, tops)]
        news = [dot(v, e.astype(BF16), 0, 0) for e in exps]
        for i in range(maps):
            m_ref[i, :, at] = tops[i]
            l_ref[i, :, at] = l_ref[i, :, at] * factors[i] + jnp.sum(exps[i], axis=0, keepdims=True)
            o_ref[i, :, at] = o_ref[i, :, at] * factors[i] + news[i]

    def mate_arrives(k):
        for q in range(CHUNKS):
            side(mate - 2 * k, q).wait_recv()

    @pl.when(z >= 1)
    def _():
        visit([s - 2])

    relays(14.8)

    @pl.when(s == 0)
    def _():
        gl[:PAD, :] = jnp.zeros((PAD, gl.shape[1]), F32)

    @pl.when(s > 0)
    def _():
        tail.wait_recv()
        gl[:PAD, :] = tail_in[...].astype(F32)

    n_taps = taps_ref.shape[0]
    taps = taps_ref[...].astype(F32)
    conv = jnp.zeros((rows, gl.shape[1]), F32)
    for j in range(n_taps):
        lo = PAD - (n_taps - 1) + j
        conv = conv + gl[lo : lo + rows, :] * taps[j : j + 1, :]
    ones = jnp.ones((8, conv.shape[1]), F32)
    high = lax.Precision.HIGHEST
    sq_out[...] = dot(ones, conv * conv, 1, 1, high)
    gl[PAD:, :] = conv
    sq_copies = [
        tp_copy(sq_out, sq_in.at[i], sq_send.at[0], sq_recv.at[i], p)
        for i, p in enumerate((p1, p2, p3))
    ]
    for copy in sq_copies:
        copy.start()
    relays(15.4)

    @pl.when(y == 1)
    def _():
        mate_arrives(0)

    @pl.when((y == 1) & (z > 0))
    def _():
        visit([mate])

    relays(100.0)

    if last_static >= 2:

        @pl.when(z == 2)
        def _():
            visit([s - 4])

    if last_static >= 3:

        @pl.when(z >= 3)
        def _():
            visit([s - 4, s - 6])

    def beyond(k, carry):
        for q in range(CHUNKS):
            relay(k, q)
        visit([s - 2 * k])
        return carry

    if nz - 1 > NEAR_STEPS:
        lax.fori_loop(NEAR_STEPS + 1, z + 1, beyond, 0)

    gate_conv = projected(5).astype(F32)
    for copy in sq_copies:
        copy.wait_recv()
    total_sq = sq_out[...] + sq_in[0] + sq_in[1] + sq_in[2]
    conv_local = gl.shape[1]
    spread = jnp.full((8, conv_local), 0.125, F32)
    mean_sq = dot(total_sq, spread, 0, 0, high) / (conv_local * n_tp)
    normed = gl[PAD:, :] * lax.rsqrt(mean_sq + EPSILON) * conv_gain[...]
    ybuf[:, :conv_local] = (
        normed * jax.nn.sigmoid(normed) * (gate_conv * jax.nn.sigmoid(gate_conv))
    ).astype(BF16)

    part = rows // n_tp
    both = 2 * part
    far_rows = pl.ds(pl.multiple_of(p2 // 2 * both, both), both)
    near_rows = pl.ds(pl.multiple_of(t // 2 * both, both), both)

    def finish(at):
        for h in range(heads):
            first_map = o_ref[2 * h, :, at] / l_ref[2 * h, :, at]
            second_map = o_ref[2 * h + 1, :, at] / l_ref[2 * h + 1, :, at]
            o = first_map - lam[:, h : h + 1] * second_map
            n = o * lax.rsqrt(jnp.mean(o * o, axis=0, keepdims=True) + EPSILON)
            n = jnp.transpose(n) * head_gain[...] * HEAD_SCALE
            lo = h * VDIM
            ybuf[at, conv_local + lo : conv_local + lo + VDIM] = (
                n * ga[at, lo : lo + VDIM]
            ).astype(BF16)

    pltpu.make_async_copy(w_out, w_out, w_sem.at[1]).wait()

    def beyond_mate(k, carry):
        mate_arrives(k)
        visit([mate - 2 * k])
        return carry

    if nz - 1 > NEAR_STEPS:
        lax.fori_loop(NEAR_STEPS + 1, z + 1, beyond_mate, 0)

    @pl.when(z >= 1)
    def _():
        mate_arrives(1)

    @pl.when(z >= 2)
    def _():
        visit([mate - 2])
        mate_arrives(2)

    if last_static >= 3:

        @pl.when(z >= 3)
        def _():
            mate_arrives(3)

    def last_mate(at):
        @pl.when((z == 0) & (y == 1))
        def _():
            visit([mate], at)

        @pl.when(z == 1)
        def _():
            visit([mate - 2], at)

        if last_static >= 2:

            @pl.when(z == 2)
            def _():
                visit([mate - 4], at)

        if last_static >= 3:

            @pl.when(z >= 3)
            def _():
                visit([mate - 4, mate - 6], at)

    last_mate(far_rows)
    finish(far_rows)

    def block(p):
        return ybuf[pl.ds(pl.multiple_of(p * part, part), part), :]

    cols = w_out.shape[1] // PIECES
    far = jnp.concatenate([block(p3), block(p2)], axis=0)
    a_copies = []
    for c in range(PIECES):
        r = dot(far, w_out[:, c * cols : (c + 1) * cols]).astype(BF16)
        a_out[c] = r[:part]
        a_own[c] = r[part:]
        copy = tp_copy(a_out.at[c], a_in.at[c], a_sem.at[0], a_sem.at[1 + c], p1)
        copy.start()
        a_copies.append(copy)
    x_copies = []
    for c in range(PIECES):
        a_copies[c].wait_recv()
        x_out[c] = (a_own[c].astype(F32) + a_in[c].astype(F32)).astype(BF16)
        copy = tp_copy(x_out.at[c], x_in.at[c], x_sem.at[0], x_sem.at[1 + c], p2)
        copy.start()
        x_copies.append(copy)
    last_mate(near_rows)
    finish(near_rows)
    near = jnp.concatenate([block(p1), block(t)], axis=0)
    b_copies = []
    for c in range(PIECES):
        r = dot(near, w_out[:, c * cols : (c + 1) * cols]).astype(BF16)
        b_out[c] = r[:part]
        b_own[c] = r[part:]
        copy = tp_copy(b_out.at[c], b_in.at[c], b_sem.at[0], b_sem.at[1 + c], p1)
        copy.start()
        b_copies.append(copy)
    def sent(ref, sem):
        pltpu.make_async_copy(ref, ref, sem).wait()

    sent(tok, tok_send.at[0])
    sent(tok, tok_send.at[1])
    sent(tok, tok_send.at[2])
    sent(sq_in, sq_send.at[0])
    sent(a_out, a_sem.at[0])

    @pl.when(s + 1 < n_sp)
    def _():
        tail.wait_send()

    @pl.when(has_up)
    def _():
        sent(kv.at[s], up_send.at[s])

    @pl.when(has_skip)
    def _():
        sent(kv.at[s], skip_send.at[0])

    @pl.when(y == 0)
    def _():
        sent(kv.at[s], side_send.at[s])

    def drain(k, carry):
        j = s - 2 * k

        @pl.when(has_up & (k != SKIP - 1))
        def _():
            sent(kv.at[j], up_send.at[j])

        sent(kv.at[j], side_send.at[j])
        return carry

    lax.fori_loop(1, z + 1, drain, 0)
    for c in range(PIECES):
        b_copies[c].wait_recv()
    for c in range(PIECES):
        x_copies[c].wait_recv()
        out[:, c * cols : (c + 1) * cols] = (
            b_own[c].astype(F32) + b_in[c].astype(F32) + x_in[c].astype(F32)
        ).astype(BF16)
    sent(x_out, x_sem.at[0])
    sent(b_out, b_sem.at[0])


def local(n_sp, n_tp, *args):
    (tokens, in_gain, w_glu_value, w_glu_gate, w_query, w_key, w_value, w_gate_conv,
     w_gate_attn, conv_weight, conv_gain, lam, head_gain, out_conv, out_attn) = args
    rows, depth = tokens.shape
    width = depth * n_tp
    weights = (w_glu_value, w_glu_gate, w_query, w_key, w_value, w_gate_conv, w_gate_attn)
    total_cols = sum(w.shape[1] for w in weights)
    out_rows = out_conv.shape[0] + out_attn.shape[0]
    out_cols = out_conv.shape[1]
    conv_local = conv_weight.shape[1]
    heads = lam.shape[0]
    part = rows // n_tp
    cols = out_cols // PIECES
    vmem = pl.BlockSpec(memory_space=pltpu.VMEM)
    hbm = pl.BlockSpec(memory_space=pl.ANY)
    dma = pltpu.SemaphoreType.DMA
    piece = pltpu.VMEM((PIECES, part, cols), BF16)
    return pl.pallas_call(
        functools.partial(kernel, n_sp, n_tp),
        out_shape=pltpu.VMEM((part, out_cols), BF16),
        in_specs=[hbm] * len(args),
        out_specs=vmem,
        scratch_shapes=[
            pltpu.VMEM((width, total_cols), BF16),
            pltpu.VMEM((out_rows, out_cols), BF16),
            pltpu.VMEM((3, rows, depth), BF16),
            pltpu.VMEM((2, rows, depth), BF16),
            pltpu.VMEM((rows, total_cols), F32),
            pltpu.VMEM((n_sp, 2, rows, VDIM), BF16),
            pltpu.VMEM((2 * heads, rows, 2 * QK), BF16),
            pltpu.VMEM((2 * heads, 1, rows), F32),
            pltpu.VMEM((2 * heads, 1, rows), F32),
            pltpu.VMEM((2 * heads, VDIM, rows), F32),
            pltpu.VMEM((PAD + rows, conv_local), F32),
            pltpu.VMEM((PAD, conv_local), BF16),
            pltpu.VMEM((PAD, conv_local), BF16),
            pltpu.VMEM((8, rows), F32),
            pltpu.VMEM((3, 8, rows), F32),
            pltpu.VMEM((rows, out_rows), BF16),
            piece, piece, piece, piece, piece, piece, piece, piece,
            dma((2,)),
            dma((3,)),
            dma((2 * CHUNKS + 1,)),
            dma((n_sp, CHUNKS)),
            dma((n_sp,)),
            dma((1,)),
            dma((n_sp,)),
            dma((2,)),
            dma((1,)),
            dma((3,)),
            dma((1 + PIECES,)),
            dma((1 + PIECES,)),
            dma((1 + PIECES,)),
            pltpu.VMEM((width // LANES, LANES), F32),
            pltpu.VMEM(tokens.shape, BF16),
            pltpu.VMEM((width // LANES, LANES), BF16),
            pltpu.VMEM(conv_weight.shape, BF16),
            pltpu.VMEM((1, conv_local), F32),
            pltpu.VMEM((1, heads), F32),
            pltpu.VMEM((1, VDIM), F32),
            pltpu.VMEM((rows, heads * VDIM), F32),
            dma((6,)),
        ],
        compiler_params=pltpu.CompilerParams(
            collective_id=0, has_side_effects=True, vmem_limit_bytes=60 * 1024 * 1024
        ),
    )(
        tokens, in_gain.reshape(width // LANES, LANES), w_glu_value, w_glu_gate, w_query, w_key, w_value,
        w_gate_conv, w_gate_attn, conv_weight, conv_gain.reshape(1, conv_local),
        lam.reshape(1, heads),
        head_gain.reshape(1, VDIM), out_conv, out_attn,
    )


def solution(mesh):
    n_sp, n_tp = mesh.shape["sp"], mesh.shape["tp"]
    assert n_tp == 4 and n_sp % 2 == 0 and 2 * QK == VDIM
    col = P(None, "tp")
    in_specs = (
        P("sp", "tp"), P(), col, col, col, col, col, col, col, col,
        P("tp"), P("tp"), P(), P("tp", None), P("tp", None),
    )
    return jax.shard_map(
        functools.partial(local, n_sp, n_tp), mesh=mesh, in_specs=in_specs,
        out_specs=P(("sp", "tp"), None), check_vma=False,
    )
```

```python
import functools
import math

import jax
import jax.numpy as jnp
from jax import lax
from jax.experimental import pallas as pl
from jax.experimental.pallas import tpu as pltpu
from jax.sharding import PartitionSpec as P

EPSILON = 1e-06
NEG_BIG = -1e30
HEAD_SCALE = 0.8
QK = 64
VDIM = 128
MESH = pl.DeviceIdType.MESH
F32 = jnp.float32
BF16 = jnp.bfloat16
PIECES = 4
PAD = 32
LANES = 128
CHUNKS = 4
NEAR_STEPS = 3
SKIP = 3
HALF = CHUNKS // 2


def dot(a, b, ca=1, cb=0, precision=None):
    return lax.dot_general(
        a, b, (((ca,), (cb,)), ((), ())), preferred_element_type=F32, precision=precision
    )


def kernel(
    n_sp,
    n_tp,
    tok_hbm,
    gain_hbm,
    w_glu_value,
    w_glu_gate,
    w_query,
    w_key,
    w_value,
    w_gate_conv,
    w_gate_attn,
    taps_hbm,
    conv_gain_hbm,
    lam_hbm,
    head_gain_hbm,
    out_conv,
    out_attn,
    out,
    w_all,
    w_out,
    tokbuf,
    scaled_far,
    acc,
    kv,
    q4,
    m_ref,
    l_ref,
    o_ref,
    gl,
    tail_out,
    tail_in,
    sq_out,
    sq_in,
    ybuf,
    a_out,
    a_own,
    a_in,
    x_out,
    x_in,
    b_out,
    b_own,
    b_in,
    w_sem,
    tok_send,
    tok_recv,
    kv_recv,
    side_recv,
    up_send,
    skip_send,
    side_send,
    tail_sem,
    sq_send,
    sq_recv,
    a_sem,
    x_sem,
    b_sem,
    gain32,
    tok,
    gain,
    taps_ref,
    conv_gain,
    lam,
    head_gain,
    ga,
    small_sem,
    near_sem,
    far_sem,
):
    rows, depth = tok.shape
    width = depth * n_tp
    s = lax.axis_index("sp")
    t = lax.axis_index("tp")
    core = t % 2
    p1 = t + 1 - 2 * core
    p2 = (t + 2) % n_tp
    p3 = (p1 + 2) % n_tp
    y = s % 2
    z = s // 2
    nz = n_sp // 2
    mate = s + 1 - 2 * y
    has_up = s + 2 < n_sp
    has_skip = s + 2 * SKIP < n_sp
    size = rows // CHUNKS
    last_static = min(NEAR_STEPS, nz - 1)

    smalls = [
        pltpu.make_async_copy(src, dst, small_sem.at[i])
        for i, (src, dst) in enumerate((
            (tok_hbm, tok), (gain_hbm, gain), (taps_hbm, taps_ref),
            (conv_gain_hbm, conv_gain), (lam_hbm, lam), (head_gain_hbm, head_gain),
        ))
    ]
    for copy in smalls:
        copy.start()
    weights = (w_key, w_value, w_glu_value, w_glu_gate, w_query, w_gate_conv, w_gate_attn)
    spans = []
    at = 0
    loads = []
    for i, w in enumerate(weights):
        cols = w.shape[1]
        spans.append((at, at + cols))
        loads.append(pltpu.make_async_copy(w, w_all.at[:, at : at + cols], w_sem.at[0]))
        at += cols
    at = 0
    out_loads = []
    for i, w in enumerate((out_conv, out_attn)):
        r = w.shape[0]
        out_loads.append(
            pltpu.make_async_copy(w, w_out.at[at : at + r, :], w_sem.at[1])
        )
        at += r

    def tp_copy(src, dst, send, recv, to):
        return pltpu.make_async_remote_copy(
            src_ref=src, dst_ref=dst, send_sem=send, recv_sem=recv,
            device_id={"tp": to}, device_id_type=MESH,
        )

    def sp_copy(src, dst, send, recv, to):
        return pltpu.make_async_remote_copy(
            src_ref=src, dst_ref=dst, send_sem=send, recv_sem=recv,
            device_id={"sp": to}, device_id_type=MESH,
        )

    barrier = pltpu.get_barrier_semaphore()
    for peer in (p1, p2, p3):
        pl.semaphore_signal(barrier, inc=1, device_id={"tp": peer}, device_id_type=MESH)
    expected = jnp.int32(3)
    for by in (1, 2):
        for other in (s - by, s + by):
            valid = (other >= 0) & (other < n_sp)
            expected = expected + valid.astype(jnp.int32)

            @pl.when(valid)
            def _():
                pl.semaphore_signal(barrier, inc=1, device_id={"sp": other}, device_id_type=MESH)

    for copy in smalls:
        copy.wait()
    for copy in loads:
        copy.start()
    pl.semaphore_wait(barrier, expected)

    def piece_rows(q):
        return slice(q * size, (q + 1) * size)

    across = [
        tp_copy(
            tok.at[piece_rows(q)], tokbuf.at[1, piece_rows(q)],
            tok_send.at[0], tok_recv.at[q], p3,
        )
        for q in range(CHUNKS)
    ]
    passed = [
        tp_copy(
            tokbuf.at[1, piece_rows(q)], tokbuf.at[2, piece_rows(q)],
            tok_send.at[1], tok_recv.at[CHUNKS + q], p1,
        )
        for q in range(CHUNKS)
    ]
    beside = tp_copy(tok, tokbuf.at[0], tok_send.at[2], tok_recv.at[2 * CHUNKS], p1)
    for copy in across:
        copy.start()
    beside.start()
    for copy in out_loads:
        copy.start()

    def tell(sem):
        pl.semaphore_signal(sem, inc=1, device_id={"sp": s - 2}, device_id_type=MESH)

    @pl.when((s >= 2) & has_up)
    def _():
        tell(near_sem)

    def sent(ref, sem):
        pltpu.make_async_copy(ref, ref, sem).wait()

    lines = depth // LANES

    def prepare(x, owner):
        wide = x.astype(F32)
        parts = [
            wide[:, b * LANES : (b + 1) * LANES] * gain32[pl.ds(owner * lines + b, 1), :]
            for b in range(lines)
        ]
        scaled = jnp.concatenate(parts, axis=1).astype(BF16)
        return scaled, jnp.sum(wide * wide, axis=1, keepdims=True)

    def w_rows(owner, lo, hi):
        return w_all[pl.ds(pl.multiple_of(owner * depth, depth), depth), lo:hi]

    first_cols = spans[3][1]
    total_cols = spans[-1][1]
    gain32[...] = gain[...].astype(F32)
    scaled_own, squares = prepare(tok[...], t)
    @pl.when(s + 4 < n_sp)
    def _():
        pl.semaphore_wait(near_sem, 1)

    @pl.when((s >= 2) & (s + 4 < n_sp))
    def _():
        tell(far_sem)

    pltpu.make_async_copy(w_all, w_all, w_sem.at[0]).wait()
    beside.wait_recv()
    scaled, more = prepare(tokbuf[0], p1)
    squares = squares + more
    acc[...] = dot(
        jnp.concatenate([scaled_own, scaled], axis=1),
        jnp.concatenate([w_rows(t, 0, total_cols), w_rows(p1, 0, total_cols)], axis=0),
    )

    def late(q):
        at = piece_rows(q)
        lhs = jnp.concatenate([scaled_far[0, at], scaled_far[1, at]], axis=1)
        rhs = jnp.concatenate(
            [w_rows(p3, first_cols, total_cols), w_rows(p2, first_cols, total_cols)], axis=0
        )
        acc[at, first_cols:] += dot(lhs, rhs)

    def chunk(j, q):
        return kv.at[j, :, piece_rows(q), :]

    def up(j, q):
        return sp_copy(chunk(j, q), chunk(j, q), up_send.at[j // 2], kv_recv.at[j // 2, q], s + 2)

    def skip(q):
        return sp_copy(chunk(s, q), chunk(s, q), skip_send.at[0], kv_recv.at[z, q], s + 2 * SKIP)

    def side(j, q):
        return sp_copy(chunk(j, q), chunk(j, q), side_send.at[j // 2], side_recv.at[j // 2, q // HALF], mate)

    def relay(k, q):
        j = s - 2 * k
        up(j, q).wait_recv()
        if isinstance(k, int):
            if k != SKIP - 1:

                @pl.when(has_up)
                def _():
                    up(j, q).start()
        else:

            @pl.when(has_up & (k != SKIP - 1))
            def _():
                up(j, q).start()

        side(j, q).start()

    def due(steps, k, q):
        if k == 1:
            return 9.9 + 1.3 * q
        return 11.3 + 1.3 * q if k == SKIP else 14.9 + 0.7 * q

    pending = {
        steps: sorted(
            ((k, q) for k in range(1, steps + 1) for q in range(CHUNKS)),
            key=lambda e: due(steps, *e),
        )
        for steps in range(1, last_static + 1)
    }

    def relays(until):
        for steps, queue in pending.items():
            now = []
            while queue and due(steps, *queue[0]) < until:
                now.append(queue.pop(0))
            if not now:
                continue

            @pl.when((z == steps) if steps < last_static else (z >= steps))
            def _():
                for k, q in now:
                    relay(k, q)

    tail = sp_copy(tail_out, tail_in, tail_sem.at[0], tail_sem.at[1], s + 1)
    inv_parts = []
    for q in range(CHUNKS):
        at = piece_rows(q)
        across[q].wait_recv()
        passed[q].start()
        scaled, sq2 = prepare(tokbuf[1, at], p3)
        scaled_far[0, at] = scaled
        part = acc[at, :first_cols] + dot(scaled, w_rows(p3, 0, first_cols))
        if q > 0:
            late(q - 1)
        passed[q].wait_recv()
        scaled, sq3 = prepare(tokbuf[2, at], p2)
        scaled_far[1, at] = scaled
        part = part + dot(scaled, w_rows(p2, 0, first_cols))
        inv = lax.rsqrt((squares[at] + sq2 + sq3) / width + EPSILON)
        inv_parts.append(inv)
        part = (part * inv).astype(BF16)

        def glue():
            value = part[:, spans[2][0] : spans[2][1]].astype(F32)
            gate = part[:, spans[3][0] : spans[3][1]].astype(F32)
            glued = (value * jax.nn.sigmoid(gate)).astype(BF16)
            gl[PAD + q * size : PAD + (q + 1) * size, :] = glued.astype(F32)
            return glued

        if q == CHUNKS - 1:
            tail_out[...] = glue()[size - PAD :]

            @pl.when(s + 1 < n_sp)
            def _():
                tail.start()

        kv[s, 0, at] = part[:, : spans[0][1]]
        kv[s, 1, at] = part[:, spans[1][0] : spans[1][1]]

        @pl.when(y == 0)
        def _():
            side(s, q).start()

        @pl.when(has_up)
        def _():
            up(s, q).start()

        @pl.when(has_skip)
        def _():
            if q == 0:
                pl.semaphore_wait(far_sem, 1)
            skip(q).start()

        if q < CHUNKS - 1:
            glue()
        relays(7.2 + 1.4 * q)
    late(CHUNKS - 1)
    inv_rms = jnp.concatenate(inv_parts, axis=0)

    def projected(i, lo=0, hi=None):
        hi = rows if hi is None else hi
        a, b = spans[i]
        return (acc[lo:hi, a:b] * inv_rms[lo:hi]).astype(BF16)

    query = projected(4).astype(F32) * (1.0 / math.sqrt(QK))
    heads = w_query.shape[1] // (2 * QK)
    maps = 2 * heads
    lane = lax.broadcasted_iota(jnp.int32, (rows, 2 * QK), 1)
    for h in range(heads):
        qh = query[:, h * 2 * QK : (h + 1) * 2 * QK]
        for m in range(2):
            keep = (lane >= m * QK) & (lane < (m + 1) * QK)
            q4[2 * h + m] = jnp.where(keep, qh, 0.0).astype(BF16)
    relays(11.9)

    key_pos = lax.broadcasted_iota(jnp.int32, (rows, rows), 0)
    query_pos = lax.broadcasted_iota(jnp.int32, (rows, rows), 1)
    allowed = key_pos <= query_pos
    k_own = kv[s, 0]
    v_own = kv[s, 1]
    scores = [jnp.where(allowed, dot(k_own, q4[i], 1, 1), NEG_BIG) for i in range(maps)]
    tops = [jnp.max(x, axis=0, keepdims=True) for x in scores]
    exps = [jnp.exp(x - top) for x, top in zip(scores, tops)]
    for i in range(maps):
        m_ref[i] = tops[i]
        l_ref[i] = jnp.sum(exps[i], axis=0, keepdims=True)
        o_ref[i] = dot(v_own, exps[i].astype(BF16), 0, 0)
    relays(12.7)

    gate_attn = projected(6).astype(F32)
    ga[...] = gate_attn * jax.nn.sigmoid(gate_attn)

    def visit(blocks, at=slice(None)):
        def stacked(plane):
            parts = [
                kv[b[0], plane, b[1] : b[2]] if isinstance(b, tuple) else kv[b, plane]
                for b in blocks
            ]
            return parts[0] if len(parts) == 1 else jnp.concatenate(parts, axis=0)

        k = stacked(0)
        v = stacked(1)
        scores = [dot(k, q4[i, at, :], 1, 1) for i in range(maps)]
        olds = [m_ref[i, :, at] for i in range(maps)]
        tops = [
            jnp.maximum(old, jnp.max(x, axis=0, keepdims=True)) for old, x in zip(olds, scores)
        ]
        exps = [jnp.exp(x - top) for x, top in zip(scores, tops)]
        factors = [jnp.exp(old - top) for old, top in zip(olds, tops)]
        news = [dot(v, e.astype(BF16), 0, 0) for e in exps]
        for i in range(maps):
            m_ref[i, :, at] = tops[i]
            l_ref[i, :, at] = l_ref[i, :, at] * factors[i] + jnp.sum(exps[i], axis=0, keepdims=True)
            o_ref[i, :, at] = o_ref[i, :, at] * factors[i] + news[i]

    middle = rows // 2

    def mate_arrives(k, halves=(0, 1)):
        for half in halves:
            ref = kv.at[mate - 2 * k, :, half * middle : (half + 1) * middle, :]
            sent(ref, side_recv.at[z - k, half])

    sq_copies = [
        tp_copy(sq_out, sq_in.at[i], sq_send.at[0], sq_recv.at[i], p)
        for i, p in enumerate((p1, p2, p3))
    ]
    high = lax.Precision.HIGHEST

    def convolve():
        @pl.when(s == 0)
        def _():
            gl[:PAD, :] = jnp.zeros((PAD, gl.shape[1]), F32)

        @pl.when(s > 0)
        def _():
            tail.wait_recv()
            gl[:PAD, :] = tail_in[...].astype(F32)

        n_taps = taps_ref.shape[0]
        taps = taps_ref[...].astype(F32)
        conv = jnp.zeros((rows, gl.shape[1]), F32)
        for j in range(n_taps):
            lo = PAD - (n_taps - 1) + j
            conv = conv + gl[lo : lo + rows, :] * taps[j : j + 1, :]
        ones = jnp.ones((8, conv.shape[1]), F32)
        sq_out[...] = dot(ones, conv * conv, 1, 1, high)
        gl[PAD:, :] = conv
        for copy in sq_copies:
            copy.start()
    @pl.when(y == 1)
    def _():
        convolve()

    relays(13.6)

    relays(14.0)

    @pl.when(z >= 1)
    def _():
        visit([s - 2])

    relays(15.3)

    @pl.when(y == 0)
    def _():
        convolve()

    relays(16.6)

    @pl.when(y == 1)
    def _():
        mate_arrives(0)

    @pl.when((y == 1) & (z > 0))
    def _():
        visit([mate])

    conv_local = gl.shape[1]
    relays(100.0)

    if last_static >= 2:

        @pl.when(z == 2)
        def _():
            visit([s - 4])

    if last_static >= 3:

        @pl.when(z >= 3)
        def _():
            visit([s - 4, s - 6])

    def beyond(k, carry):
        for q in range(CHUNKS):
            relay(k, q)
        visit([s - 2 * k])
        return carry

    if nz - 1 > NEAR_STEPS:
        lax.fori_loop(NEAR_STEPS + 1, z + 1, beyond, 0)

    conv_local = gl.shape[1]
    gate_conv = projected(5).astype(F32)
    for copy in sq_copies:
        copy.wait_recv()
    total_sq = sq_out[...] + sq_in[0] + sq_in[1] + sq_in[2]
    spread = jnp.full((8, conv_local), 0.125, F32)
    mean_sq = dot(total_sq, spread, 0, 0, high) / (conv_local * n_tp)
    normed = gl[PAD:, :] * lax.rsqrt(mean_sq + EPSILON) * conv_gain[...]
    ybuf[:, :conv_local] = (
        normed * jax.nn.sigmoid(normed) * (gate_conv * jax.nn.sigmoid(gate_conv))
    ).astype(BF16)

    part = rows // n_tp
    both = 2 * part
    far_rows = pl.ds(pl.multiple_of(p2 // 2 * both, both), both)
    near_rows = pl.ds(pl.multiple_of(t // 2 * both, both), both)

    def finish(at):
        for h in range(heads):
            first_map = o_ref[2 * h, :, at] / l_ref[2 * h, :, at]
            second_map = o_ref[2 * h + 1, :, at] / l_ref[2 * h + 1, :, at]
            o = first_map - lam[:, h : h + 1] * second_map
            n = o * lax.rsqrt(jnp.mean(o * o, axis=0, keepdims=True) + EPSILON)
            n = jnp.transpose(n) * head_gain[...] * HEAD_SCALE
            lo = h * VDIM
            ybuf[at, conv_local + lo : conv_local + lo + VDIM] = (
                n * ga[at, lo : lo + VDIM]
            ).astype(BF16)

    pltpu.make_async_copy(w_out, w_out, w_sem.at[1]).wait()

    def beyond_mate(k, carry):
        mate_arrives(k)
        visit([mate - 2 * k])
        return carry

    if nz - 1 > NEAR_STEPS:
        lax.fori_loop(NEAR_STEPS + 1, z + 1, beyond_mate, 0)

    @pl.when(z >= 1)
    def _():
        mate_arrives(1)

    if last_static >= 2:

        @pl.when(z >= 2)
        def _():
            visit([mate - 2])

    if last_static >= 3:

        @pl.when(z >= 3)
        def _():
            mate_arrives(3)
            visit([mate - 6])

    if last_static >= 2:

        @pl.when(z >= 2)
        def _():
            mate_arrives(2, (0,))
            visit([(mate - 4, 0, middle)])
            mate_arrives(2, (1,))

    def last_mate(at):
        @pl.when((z == 0) & (y == 1))
        def _():
            visit([mate], at)

        @pl.when(z == 1)
        def _():
            visit([mate - 2], at)

        if last_static >= 2:

            @pl.when(z >= 2)
            def _():
                visit([(mate - 4, middle, rows)], at)

    last_mate(far_rows)
    finish(far_rows)

    def block(p):
        return ybuf[pl.ds(pl.multiple_of(p * part, part), part), :]

    cols = w_out.shape[1] // PIECES
    far = jnp.concatenate([block(p2), block(p3)], axis=0)
    a_copies = []
    for c in range(PIECES):
        r = dot(far, w_out[:, c * cols : (c + 1) * cols]).astype(BF16)
        a_out[c] = r[:part]
        a_own[c] = r[part:]
        copy = tp_copy(a_out.at[c], a_in.at[c], a_sem.at[0], a_sem.at[1 + c], p1)
        copy.start()
        a_copies.append(copy)
    x_copies = []
    for c in range(PIECES):
        a_copies[c].wait_recv()
        x_out[c] = (a_own[c].astype(F32) + a_in[c].astype(F32)).astype(BF16)
        copy = tp_copy(x_out.at[c], x_in.at[c], x_sem.at[0], x_sem.at[1 + c], p3)
        copy.start()
        x_copies.append(copy)
    last_mate(near_rows)
    finish(near_rows)
    near = jnp.concatenate([block(p1), block(t)], axis=0)
    b_copies = []
    for c in range(PIECES):
        r = dot(near, w_out[:, c * cols : (c + 1) * cols]).astype(BF16)
        b_out[c] = r[:part]
        b_own[c] = r[part:]
        copy = tp_copy(b_out.at[c], b_in.at[c], b_sem.at[0], b_sem.at[1 + c], p1)
        copy.start()
        b_copies.append(copy)
    sent(tok, tok_send.at[0])
    sent(tok, tok_send.at[1])
    sent(tok, tok_send.at[2])
    sent(sq_in, sq_send.at[0])
    sent(a_out, a_sem.at[0])

    @pl.when(s + 1 < n_sp)
    def _():
        tail.wait_send()

    @pl.when(has_up)
    def _():
        sent(kv.at[s], up_send.at[z])

    @pl.when(has_skip)
    def _():
        sent(kv.at[s], skip_send.at[0])

    @pl.when(y == 0)
    def _():
        sent(kv.at[s], side_send.at[z])

    def drain(k, carry):
        j = s - 2 * k

        @pl.when(has_up & (k != SKIP - 1))
        def _():
            sent(kv.at[j], up_send.at[z - k])

        sent(kv.at[j], side_send.at[z - k])
        return carry

    lax.fori_loop(1, z + 1, drain, 0)
    for c in range(PIECES):
        b_copies[c].wait_recv()
    for c in range(PIECES):
        x_copies[c].wait_recv()
        out[:, c * cols : (c + 1) * cols] = (
            b_own[c].astype(F32) + b_in[c].astype(F32) + x_in[c].astype(F32)
        ).astype(BF16)
    sent(x_out, x_sem.at[0])
    sent(b_out, b_sem.at[0])


def local(n_sp, n_tp, *args):
    (tokens, in_gain, w_glu_value, w_glu_gate, w_query, w_key, w_value, w_gate_conv,
     w_gate_attn, conv_weight, conv_gain, lam, head_gain, out_conv, out_attn) = args
    rows, depth = tokens.shape
    width = depth * n_tp
    weights = (w_glu_value, w_glu_gate, w_query, w_key, w_value, w_gate_conv, w_gate_attn)
    total_cols = sum(w.shape[1] for w in weights)
    out_rows = out_conv.shape[0] + out_attn.shape[0]
    out_cols = out_conv.shape[1]
    conv_local = conv_weight.shape[1]
    heads = lam.shape[0]
    part = rows // n_tp
    cols = out_cols // PIECES
    vmem = pl.BlockSpec(memory_space=pltpu.VMEM)
    hbm = pl.BlockSpec(memory_space=pl.ANY)
    dma = pltpu.SemaphoreType.DMA
    piece = pltpu.VMEM((PIECES, part, cols), BF16)
    return pl.pallas_call(
        functools.partial(kernel, n_sp, n_tp),
        out_shape=pltpu.VMEM((part, out_cols), BF16),
        in_specs=[hbm] * len(args),
        out_specs=vmem,
        scratch_shapes=[
            pltpu.VMEM((width, total_cols), BF16),
            pltpu.VMEM((out_rows, out_cols), BF16),
            pltpu.VMEM((3, rows, depth), BF16),
            pltpu.VMEM((2, rows, depth), BF16),
            pltpu.VMEM((rows, total_cols), F32),
            pltpu.VMEM((n_sp, 2, rows, VDIM), BF16),
            pltpu.VMEM((2 * heads, rows, 2 * QK), BF16),
            pltpu.VMEM((2 * heads, 1, rows), F32),
            pltpu.VMEM((2 * heads, 1, rows), F32),
            pltpu.VMEM((2 * heads, VDIM, rows), F32),
            pltpu.VMEM((PAD + rows, conv_local), F32),
            pltpu.VMEM((PAD, conv_local), BF16),
            pltpu.VMEM((PAD, conv_local), BF16),
            pltpu.VMEM((8, rows), F32),
            pltpu.VMEM((3, 8, rows), F32),
            pltpu.VMEM((rows, out_rows), BF16),
            piece, piece, piece, piece, piece, piece, piece, piece,
            dma((2,)),
            dma((3,)),
            dma((2 * CHUNKS + 1,)),
            dma((n_sp // 2, CHUNKS)),
            dma((n_sp // 2, 2)),
            dma((n_sp // 2,)),
            dma((1,)),
            dma((n_sp // 2,)),
            dma((2,)),
            dma((1,)),
            dma((3,)),
            dma((1 + PIECES,)),
            dma((1 + PIECES,)),
            dma((1 + PIECES,)),
            pltpu.VMEM((width // LANES, LANES), F32),
            pltpu.VMEM(tokens.shape, BF16),
            pltpu.VMEM((width // LANES, LANES), BF16),
            pltpu.VMEM(conv_weight.shape, BF16),
            pltpu.VMEM((1, conv_local), F32),
            pltpu.VMEM((1, heads), F32),
            pltpu.VMEM((1, VDIM), F32),
            pltpu.VMEM((rows, heads * VDIM), F32),
            dma((6,)),
            pltpu.SemaphoreType.REGULAR,
            pltpu.SemaphoreType.REGULAR,
        ],
        compiler_params=pltpu.CompilerParams(
            collective_id=0, has_side_effects=True, vmem_limit_bytes=60 * 1024 * 1024
        ),
    )(
        tokens, in_gain.reshape(width // LANES, LANES), w_glu_value, w_glu_gate, w_query, w_key, w_value,
        w_gate_conv, w_gate_attn, conv_weight, conv_gain.reshape(1, conv_local),
        lam.reshape(1, heads),
        head_gain.reshape(1, VDIM), out_conv, out_attn,
    )


def solution(mesh):
    n_sp, n_tp = mesh.shape["sp"], mesh.shape["tp"]
    assert n_tp == 4 and n_sp % 2 == 0 and 2 * QK == VDIM
    col = P(None, "tp")
    in_specs = (
        P("sp", "tp"), P(), col, col, col, col, col, col, col, col,
        P("tp"), P("tp"), P(), P("tp", None), P("tp", None),
    )
    return jax.shard_map(
        functools.partial(local, n_sp, n_tp), mesh=mesh, in_specs=in_specs,
        out_specs=P(("sp", "tp"), None), check_vma=False,
    )
```

```python
import functools
import math

import jax
import jax.numpy as jnp
from jax import lax
from jax.experimental import pallas as pl
from jax.experimental.pallas import tpu as pltpu
from jax.sharding import PartitionSpec as P

EPSILON = 1e-06
NEG_BIG = -1e30
HEAD_SCALE = 0.8
QK = 64
VDIM = 128
MESH = pl.DeviceIdType.MESH
F32 = jnp.float32
BF16 = jnp.bfloat16
PIECES = 4
LEAD = 256
PAD = 32
LANES = 128
CHUNKS = 4
NEAR_STEPS = 3
SKIP = 3
HALF = CHUNKS // 2


def dot(a, b, ca=1, cb=0, precision=None):
    return lax.dot_general(
        a, b, (((ca,), (cb,)), ((), ())), preferred_element_type=F32, precision=precision
    )


def kernel(
    n_sp,
    n_tp,
    tok_hbm,
    gain_hbm,
    w_glu_value,
    w_glu_gate,
    w_query,
    w_key,
    w_value,
    w_gate_conv,
    w_gate_attn,
    taps_hbm,
    conv_gain_hbm,
    lam_hbm,
    head_gain_hbm,
    out_conv,
    out_attn,
    out,
    w_all,
    w_out,
    tokbuf,
    scaled_far,
    acc,
    kv,
    q4,
    m_ref,
    l_ref,
    o_ref,
    gl,
    tail_out,
    tail_in,
    sq_out,
    sq_in,
    ybuf,
    a_out,
    a_own,
    a_in,
    x_out,
    x_in,
    b_out,
    b_own,
    b_in,
    d_out,
    d_in,
    w_sem,
    tok_send,
    tok_recv,
    kv_recv,
    side_recv,
    up_send,
    skip_send,
    side_send,
    tail_sem,
    sq_send,
    sq_recv,
    a_sem,
    x_sem,
    b_sem,
    d_sem,
    gain32,
    tok,
    gain,
    taps_ref,
    conv_gain,
    lam,
    head_gain,
    ga,
    small_sem,
    near_sem,
    far_sem,
):
    rows, depth = tok.shape
    width = depth * n_tp
    s = lax.axis_index("sp")
    t = lax.axis_index("tp")
    core = t % 2
    p1 = t + 1 - 2 * core
    p2 = (t + 2) % n_tp
    p3 = (p1 + 2) % n_tp
    y = s % 2
    z = s // 2
    nz = n_sp // 2
    mate = s + 1 - 2 * y
    has_up = s + 2 < n_sp
    has_skip = s + 2 * SKIP < n_sp
    size = rows // CHUNKS
    last_static = min(NEAR_STEPS, nz - 1)

    smalls = [
        pltpu.make_async_copy(src, dst, small_sem.at[i])
        for i, (src, dst) in enumerate((
            (tok_hbm, tok), (gain_hbm, gain), (taps_hbm, taps_ref),
            (conv_gain_hbm, conv_gain), (lam_hbm, lam), (head_gain_hbm, head_gain),
        ))
    ]
    for copy in smalls:
        copy.start()
    weights = (w_key, w_value, w_glu_value, w_glu_gate, w_query, w_gate_conv, w_gate_attn)
    spans = []
    at = 0
    loads = []
    for i, w in enumerate(weights):
        cols = w.shape[1]
        spans.append((at, at + cols))
        loads.append(pltpu.make_async_copy(w, w_all.at[:, at : at + cols], w_sem.at[0]))
        at += cols
    at = 0
    out_loads = []
    for i, w in enumerate((out_conv, out_attn)):
        r = w.shape[0]
        out_loads.append(
            pltpu.make_async_copy(w, w_out.at[at : at + r, :], w_sem.at[1])
        )
        at += r

    def tp_copy(src, dst, send, recv, to):
        return pltpu.make_async_remote_copy(
            src_ref=src, dst_ref=dst, send_sem=send, recv_sem=recv,
            device_id={"tp": to}, device_id_type=MESH,
        )

    def sp_copy(src, dst, send, recv, to):
        return pltpu.make_async_remote_copy(
            src_ref=src, dst_ref=dst, send_sem=send, recv_sem=recv,
            device_id={"sp": to}, device_id_type=MESH,
        )

    barrier = pltpu.get_barrier_semaphore()
    for peer in (p1, p2, p3):
        pl.semaphore_signal(barrier, inc=1, device_id={"tp": peer}, device_id_type=MESH)
    expected = jnp.int32(3)
    for by in (1, 2):
        for other in (s - by, s + by):
            valid = (other >= 0) & (other < n_sp)
            expected = expected + valid.astype(jnp.int32)

            @pl.when(valid)
            def _():
                pl.semaphore_signal(barrier, inc=1, device_id={"sp": other}, device_id_type=MESH)

    for copy in smalls:
        copy.wait()
    for copy in loads:
        copy.start()
    pl.semaphore_wait(barrier, expected)

    def piece_rows(q):
        return slice(q * size, (q + 1) * size)

    across = [
        tp_copy(
            tok.at[piece_rows(q)], tokbuf.at[1, piece_rows(q)],
            tok_send.at[0], tok_recv.at[q], p3,
        )
        for q in range(CHUNKS)
    ]
    passed = [
        tp_copy(
            tokbuf.at[1, piece_rows(q)], tokbuf.at[2, piece_rows(q)],
            tok_send.at[1], tok_recv.at[CHUNKS + q], p1,
        )
        for q in range(CHUNKS)
    ]
    beside = tp_copy(tok, tokbuf.at[0], tok_send.at[2], tok_recv.at[2 * CHUNKS], p1)
    across[0].start()
    beside.start()

    @pl.when(core == 0)
    def _():
        for copy in across[1:]:
            copy.start()

    for copy in out_loads:
        copy.start()

    def tell(sem):
        pl.semaphore_signal(sem, inc=1, device_id={"sp": s - 2}, device_id_type=MESH)

    @pl.when((s >= 2) & has_up)
    def _():
        tell(near_sem)

    def sent(ref, sem):
        pltpu.make_async_copy(ref, ref, sem).wait()

    lines = depth // LANES

    def prepare(x, owner):
        wide = x.astype(F32)
        parts = [
            wide[:, b * LANES : (b + 1) * LANES] * gain32[pl.ds(owner * lines + b, 1), :]
            for b in range(lines)
        ]
        scaled = jnp.concatenate(parts, axis=1).astype(BF16)
        return scaled, jnp.sum(wide * wide, axis=1, keepdims=True)

    def w_rows(owner, lo, hi):
        return w_all[pl.ds(pl.multiple_of(owner * depth, depth), depth), lo:hi]

    first_cols = spans[3][1]
    total_cols = spans[-1][1]
    gain32[...] = gain[...].astype(F32)
    scaled_own, squares = prepare(tok[...], t)
    @pl.when(s + 4 < n_sp)
    def _():
        pl.semaphore_wait(near_sem, 1)

    @pl.when((s >= 2) & (s + 4 < n_sp))
    def _():
        tell(far_sem)

    pltpu.make_async_copy(w_all, w_all, w_sem.at[0]).wait()

    @pl.when(core == 1)
    def _():
        for copy in across[1:]:
            copy.start()

    beside.wait_recv()
    scaled, more = prepare(tokbuf[0], p1)
    squares = squares + more
    acc[...] = dot(
        jnp.concatenate([scaled_own, scaled], axis=1),
        jnp.concatenate([w_rows(t, 0, total_cols), w_rows(p1, 0, total_cols)], axis=0),
    )

    def late(q):
        at = piece_rows(q)
        lhs = jnp.concatenate([scaled_far[0, at], scaled_far[1, at]], axis=1)
        rhs = jnp.concatenate(
            [w_rows(p3, first_cols, total_cols), w_rows(p2, first_cols, total_cols)], axis=0
        )
        acc[at, first_cols:] += dot(lhs, rhs)

    def chunk(j, q):
        return kv.at[j, :, piece_rows(q), :]

    def up(j, q):
        return sp_copy(chunk(j, q), chunk(j, q), up_send.at[j // 2], kv_recv.at[j // 2, q], s + 2)

    def skip(q):
        return sp_copy(chunk(s, q), chunk(s, q), skip_send.at[0], kv_recv.at[z, q], s + 2 * SKIP)

    def side(j, q):
        return sp_copy(chunk(j, q), chunk(j, q), side_send.at[j // 2], side_recv.at[j // 2, q // HALF], mate)

    def relay(k, q):
        j = s - 2 * k
        up(j, q).wait_recv()
        if isinstance(k, int):
            if k != SKIP - 1:

                @pl.when(has_up)
                def _():
                    up(j, q).start()
        else:

            @pl.when(has_up & (k != SKIP - 1))
            def _():
                up(j, q).start()

        side(j, q).start()

    def due(steps, k, q):
        if k == 1:
            return 9.9 + 1.43 * q
        return 11.3 + 1.3 * q if k == SKIP else 14.9 + 0.7 * q

    pending = {
        steps: sorted(
            ((k, q) for k in range(1, steps + 1) for q in range(CHUNKS)),
            key=lambda e: due(steps, *e),
        )
        for steps in range(1, last_static + 1)
    }

    for queue in pending.values():
        queue.remove((1, 0))

    def relays(until):
        for steps, queue in pending.items():
            now = []
            while queue and due(steps, *queue[0]) < until:
                now.append(queue.pop(0))
            if not now:
                continue

            @pl.when((z == steps) if steps < last_static else (z >= steps))
            def _():
                for k, q in now:
                    relay(k, q)

    tail = sp_copy(tail_out, tail_in, tail_sem.at[0], tail_sem.at[1], s + 1)
    inv_parts = []
    for q in range(CHUNKS):
        at = piece_rows(q)
        across[q].wait_recv()
        passed[q].start()
        scaled, sq2 = prepare(tokbuf[1, at], p3)
        scaled_far[0, at] = scaled
        part = acc[at, :first_cols] + dot(scaled, w_rows(p3, 0, first_cols))
        if q > 0:
            late(q - 1)
        passed[q].wait_recv()
        scaled, sq3 = prepare(tokbuf[2, at], p2)
        scaled_far[1, at] = scaled
        part = part + dot(scaled, w_rows(p2, 0, first_cols))
        inv = lax.rsqrt((squares[at] + sq2 + sq3) / width + EPSILON)
        inv_parts.append(inv)
        part = (part * inv).astype(BF16)

        def glue():
            value = part[:, spans[2][0] : spans[2][1]].astype(F32)
            gate = part[:, spans[3][0] : spans[3][1]].astype(F32)
            glued = (value * jax.nn.sigmoid(gate)).astype(BF16)
            gl[PAD + q * size : PAD + (q + 1) * size, :] = glued.astype(F32)
            return glued

        if q == CHUNKS - 1:
            tail_out[...] = glue()[size - PAD :]

            @pl.when(s + 1 < n_sp)
            def _():
                tail.start()

        kv[s, 0, at] = part[:, : spans[0][1]]
        kv[s, 1, at] = part[:, spans[1][0] : spans[1][1]]

        @pl.when(y == 0)
        def _():
            side(s, q).start()

        @pl.when(has_up)
        def _():
            up(s, q).start()

        @pl.when(has_skip)
        def _():
            if q == 0:
                pl.semaphore_wait(far_sem, 1)
            skip(q).start()

        if q < CHUNKS - 1:
            glue()
        if q == CHUNKS - 2:

            @pl.when((z >= 1) & (core == 1))
            def _():
                relay(1, 0)

        if q == CHUNKS - 1:

            @pl.when((z >= 1) & (core == 0))
            def _():
                relay(1, 0)

        relays(7.2 + 1.4 * q)
    late(CHUNKS - 1)
    inv_rms = jnp.concatenate(inv_parts, axis=0)

    def projected(i, lo=0, hi=None):
        hi = rows if hi is None else hi
        a, b = spans[i]
        return (acc[lo:hi, a:b] * inv_rms[lo:hi]).astype(BF16)

    query = projected(4).astype(F32) * (1.0 / math.sqrt(QK))
    heads = w_query.shape[1] // (2 * QK)
    maps = 2 * heads
    lane = lax.broadcasted_iota(jnp.int32, (rows, 2 * QK), 1)
    for h in range(heads):
        qh = query[:, h * 2 * QK : (h + 1) * 2 * QK]
        for m in range(2):
            keep = (lane >= m * QK) & (lane < (m + 1) * QK)
            q4[2 * h + m] = jnp.where(keep, qh, 0.0).astype(BF16)
    relays(11.9)

    key_pos = lax.broadcasted_iota(jnp.int32, (rows, rows), 0)
    query_pos = lax.broadcasted_iota(jnp.int32, (rows, rows), 1)
    allowed = key_pos <= query_pos
    k_own = kv[s, 0]
    v_own = kv[s, 1]
    scores = [jnp.where(allowed, dot(k_own, q4[i], 1, 1), NEG_BIG) for i in range(maps)]
    tops = [jnp.max(x, axis=0, keepdims=True) for x in scores]
    exps = [jnp.exp(x - top) for x, top in zip(scores, tops)]
    for i in range(maps):
        m_ref[i] = tops[i]
        l_ref[i] = jnp.sum(exps[i], axis=0, keepdims=True)
        o_ref[i] = dot(v_own, exps[i].astype(BF16), 0, 0)
    relays(12.8)

    gate_attn = projected(6).astype(F32)
    ga[...] = gate_attn * jax.nn.sigmoid(gate_attn)

    def visit(blocks, at=slice(None)):
        def stacked(plane):
            parts = [
                kv[b[0], plane, b[1] : b[2]] if isinstance(b, tuple) else kv[b, plane]
                for b in blocks
            ]
            return parts[0] if len(parts) == 1 else jnp.concatenate(parts, axis=0)

        k = stacked(0)
        v = stacked(1)
        scores = [dot(k, q4[i, at, :], 1, 1) for i in range(maps)]
        olds = [m_ref[i, :, at] for i in range(maps)]
        tops = [
            jnp.maximum(old, jnp.max(x, axis=0, keepdims=True)) for old, x in zip(olds, scores)
        ]
        exps = [jnp.exp(x - top) for x, top in zip(scores, tops)]
        factors = [jnp.exp(old - top) for old, top in zip(olds, tops)]
        news = [dot(v, e.astype(BF16), 0, 0) for e in exps]
        for i in range(maps):
            m_ref[i, :, at] = tops[i]
            l_ref[i, :, at] = l_ref[i, :, at] * factors[i] + jnp.sum(exps[i], axis=0, keepdims=True)
            o_ref[i, :, at] = o_ref[i, :, at] * factors[i] + news[i]

    middle = rows // 2

    def mate_arrives(k, halves=(0, 1)):
        for half in halves:
            ref = kv.at[mate - 2 * k, :, half * middle : (half + 1) * middle, :]
            sent(ref, side_recv.at[z - k, half])

    sq_copies = [
        tp_copy(sq_out, sq_in.at[i], sq_send.at[0], sq_recv.at[i], p)
        for i, p in enumerate((p1, p2, p3))
    ]
    high = lax.Precision.HIGHEST

    def convolve():
        @pl.when(s == 0)
        def _():
            gl[:PAD, :] = jnp.zeros((PAD, gl.shape[1]), F32)

        @pl.when(s > 0)
        def _():
            tail.wait_recv()
            gl[:PAD, :] = tail_in[...].astype(F32)

        n_taps = taps_ref.shape[0]
        taps = taps_ref[...].astype(F32)
        conv = jnp.zeros((rows, gl.shape[1]), F32)
        for j in range(n_taps):
            lo = PAD - (n_taps - 1) + j
            conv = conv + gl[lo : lo + rows, :] * taps[j : j + 1, :]
        ones = jnp.ones((8, conv.shape[1]), F32)
        sq_out[...] = dot(ones, conv * conv, 1, 1, high)
        gl[PAD:, :] = conv
        for copy in sq_copies:
            copy.start()
    @pl.when(y == 1)
    def _():
        convolve()

    relays(14.01)

    relays(15.25)

    @pl.when(z >= 1)
    def _():
        visit([s - 2])

    relays(15.3)

    @pl.when(y == 0)
    def _():
        convolve()

    relays(16.6)

    @pl.when(y == 1)
    def _():
        mate_arrives(0)

    @pl.when((y == 1) & (z > 0))
    def _():
        visit([mate])

    conv_local = gl.shape[1]
    relays(100.0)

    if last_static >= 2:

        @pl.when(z == 2)
        def _():
            visit([s - 4])

    if last_static >= 3:

        @pl.when(z >= 3)
        def _():
            visit([s - 4, s - 6])

    def beyond(k, carry):
        for q in range(CHUNKS):
            relay(k, q)
        visit([s - 2 * k])
        return carry

    if nz - 1 > NEAR_STEPS:
        lax.fori_loop(NEAR_STEPS + 1, z + 1, beyond, 0)

    conv_local = gl.shape[1]
    gate_conv = projected(5).astype(F32)
    for copy in sq_copies:
        copy.wait_recv()
    total_sq = sq_out[...] + sq_in[0] + sq_in[1] + sq_in[2]
    spread = jnp.full((8, conv_local), 0.125, F32)
    mean_sq = dot(total_sq, spread, 0, 0, high) / (conv_local * n_tp)
    normed = gl[PAD:, :] * lax.rsqrt(mean_sq + EPSILON) * conv_gain[...]
    ybuf[:, :conv_local] = (
        normed * jax.nn.sigmoid(normed) * (gate_conv * jax.nn.sigmoid(gate_conv))
    ).astype(BF16)

    part = rows // n_tp
    both = 2 * part
    far_rows = pl.ds(pl.multiple_of(p2 // 2 * both, both), both)
    near_rows = pl.ds(pl.multiple_of(t // 2 * both, both), both)

    def finish(at):
        for h in range(heads):
            first_map = o_ref[2 * h, :, at] / l_ref[2 * h, :, at]
            second_map = o_ref[2 * h + 1, :, at] / l_ref[2 * h + 1, :, at]
            o = first_map - lam[:, h : h + 1] * second_map
            n = o * lax.rsqrt(jnp.mean(o * o, axis=0, keepdims=True) + EPSILON)
            n = jnp.transpose(n) * head_gain[...] * HEAD_SCALE
            lo = h * VDIM
            ybuf[at, conv_local + lo : conv_local + lo + VDIM] = (
                n * ga[at, lo : lo + VDIM]
            ).astype(BF16)

    pltpu.make_async_copy(w_out, w_out, w_sem.at[1]).wait()

    def beyond_mate(k, carry):
        mate_arrives(k)
        visit([mate - 2 * k])
        return carry

    if nz - 1 > NEAR_STEPS:
        lax.fori_loop(NEAR_STEPS + 1, z + 1, beyond_mate, 0)

    @pl.when(z >= 1)
    def _():
        mate_arrives(1)

    if last_static >= 2:

        @pl.when(z >= 2)
        def _():
            visit([mate - 2])

    if last_static >= 3:

        @pl.when(z >= 3)
        def _():
            mate_arrives(3)
            visit([mate - 6])

    if last_static >= 2:

        @pl.when(z >= 2)
        def _():
            mate_arrives(2, (0,))
            visit([(mate - 4, 0, middle)])
            mate_arrives(2, (1,))

    def last_mate(at):
        @pl.when((z == 0) & (y == 1))
        def _():
            visit([mate], at)

        @pl.when(z == 1)
        def _():
            visit([mate - 2], at)

        if last_static >= 2:

            @pl.when(z >= 2)
            def _():
                visit([(mate - 4, middle, rows)], at)

    last_mate(far_rows)
    finish(far_rows)

    def block(p):
        return ybuf[pl.ds(pl.multiple_of(p * part, part), part), :]

    width_out = w_out.shape[1]
    lanes = (width_out - LEAD) // LANES
    edges = [LEAD + LANES * (lanes * c // PIECES) for c in range(PIECES + 1)]
    ranges = [slice(lo, hi) for lo, hi in zip(edges, edges[1:])]
    lead = slice(0, LEAD)
    far = jnp.concatenate([block(p2), block(p3)], axis=0)
    r = dot(far, w_out[:, lead]).astype(BF16)
    x_out[:, lead] = r[part:]
    d_out[...] = r[:part]
    direct = [
        tp_copy(x_out.at[:, lead], x_in.at[:, lead], x_sem.at[1], x_sem.at[2], p3),
        tp_copy(d_out, d_in, d_sem.at[0], d_sem.at[1], p2),
    ]
    for copy in direct:
        copy.start()
    a_copies = []
    for c, at in enumerate(ranges):
        r = dot(far, w_out[:, at]).astype(BF16)
        a_out[:, at] = r[:part]
        a_own[:, at] = r[part:]
        copy = tp_copy(a_out.at[:, at], a_in.at[:, at], a_sem.at[0], a_sem.at[1 + c], p1)
        copy.start()
        a_copies.append(copy)
    x_copies = []
    for c, at in enumerate(ranges):
        a_copies[c].wait_recv()
        x_out[:, at] = (a_own[:, at].astype(F32) + a_in[:, at].astype(F32)).astype(BF16)
        copy = tp_copy(x_out.at[:, at], x_in.at[:, at], x_sem.at[0], x_sem.at[3 + c], p3)
        copy.start()
        x_copies.append(copy)
    last_mate(near_rows)
    finish(near_rows)
    near = jnp.concatenate([block(p1), block(t)], axis=0)
    half_out = width_out // 2
    for c in range(2):
        at = slice(c * half_out, (c + 1) * half_out)
        r = dot(near, w_out[:, at]).astype(BF16)
        b_out[:, at] = r[:part]
        b_own[:, at] = r[part:].astype(F32)
    b_copy = tp_copy(b_out, b_in, b_sem.at[0], b_sem.at[1], p1)
    b_copy.start()
    sent(tok, tok_send.at[0])
    sent(tok, tok_send.at[1])
    sent(tok, tok_send.at[2])
    sent(sq_in, sq_send.at[0])
    sent(a_out.at[:, LEAD:], a_sem.at[0])

    @pl.when(s + 1 < n_sp)
    def _():
        tail.wait_send()

    @pl.when(has_up)
    def _():
        sent(kv.at[s], up_send.at[z])

    @pl.when(has_skip)
    def _():
        sent(kv.at[s], skip_send.at[0])

    @pl.when(y == 0)
    def _():
        sent(kv.at[s], side_send.at[z])

    def drain(k, carry):
        j = s - 2 * k

        @pl.when(has_up & (k != SKIP - 1))
        def _():
            sent(kv.at[j], up_send.at[z - k])

        sent(kv.at[j], side_send.at[z - k])
        return carry

    lax.fori_loop(1, z + 1, drain, 0)
    b_copy.wait_recv()
    b_own[...] = (b_own[...].astype(F32) + b_in[...].astype(F32))
    for copy in direct:
        copy.wait_recv()
    out[:, lead] = (
        b_own[:, lead] + x_in[:, lead].astype(F32) + d_in[...].astype(F32)
    ).astype(BF16)
    for c, at in enumerate(ranges):
        x_copies[c].wait_recv()
        out[:, at] = (b_own[:, at] + x_in[:, at].astype(F32)).astype(BF16)
    for copy in direct:
        copy.wait_send()
    sent(x_out.at[:, LEAD:], x_sem.at[0])
    sent(b_out, b_sem.at[0])


def local(n_sp, n_tp, *args):
    (tokens, in_gain, w_glu_value, w_glu_gate, w_query, w_key, w_value, w_gate_conv,
     w_gate_attn, conv_weight, conv_gain, lam, head_gain, out_conv, out_attn) = args
    rows, depth = tokens.shape
    width = depth * n_tp
    weights = (w_glu_value, w_glu_gate, w_query, w_key, w_value, w_gate_conv, w_gate_attn)
    total_cols = sum(w.shape[1] for w in weights)
    out_rows = out_conv.shape[0] + out_attn.shape[0]
    out_cols = out_conv.shape[1]
    conv_local = conv_weight.shape[1]
    heads = lam.shape[0]
    part = rows // n_tp
    vmem = pl.BlockSpec(memory_space=pltpu.VMEM)
    hbm = pl.BlockSpec(memory_space=pl.ANY)
    dma = pltpu.SemaphoreType.DMA
    piece = pltpu.VMEM((part, out_cols), BF16)
    return pl.pallas_call(
        functools.partial(kernel, n_sp, n_tp),
        out_shape=pltpu.VMEM((part, out_cols), BF16),
        in_specs=[hbm] * len(args),
        out_specs=vmem,
        scratch_shapes=[
            pltpu.VMEM((width, total_cols), BF16),
            pltpu.VMEM((out_rows, out_cols), BF16),
            pltpu.VMEM((3, rows, depth), BF16),
            pltpu.VMEM((2, rows, depth), BF16),
            pltpu.VMEM((rows, total_cols), F32),
            pltpu.VMEM((n_sp, 2, rows, VDIM), BF16),
            pltpu.VMEM((2 * heads, rows, 2 * QK), BF16),
            pltpu.VMEM((2 * heads, 1, rows), F32),
            pltpu.VMEM((2 * heads, 1, rows), F32),
            pltpu.VMEM((2 * heads, VDIM, rows), F32),
            pltpu.VMEM((PAD + rows, conv_local), F32),
            pltpu.VMEM((PAD, conv_local), BF16),
            pltpu.VMEM((PAD, conv_local), BF16),
            pltpu.VMEM((8, rows), F32),
            pltpu.VMEM((3, 8, rows), F32),
            pltpu.VMEM((rows, out_rows), BF16),
            piece, piece, piece, piece, piece, piece,
            pltpu.VMEM((part, out_cols), F32),
            piece,
            pltpu.VMEM((part, LEAD), BF16),
            pltpu.VMEM((part, LEAD), BF16),
            dma((2,)),
            dma((3,)),
            dma((2 * CHUNKS + 1,)),
            dma((max(n_sp // 2 - 1, 1), CHUNKS)),
            dma((n_sp // 2, 2)),
            dma((n_sp // 2,)),
            dma((1,)),
            dma((n_sp // 2,)),
            dma((2,)),
            dma((1,)),
            dma((3,)),
            dma((1 + PIECES,)),
            dma((3 + PIECES,)),
            dma((2,)),
            dma((2,)),
            pltpu.VMEM((width // LANES, LANES), F32),
            pltpu.VMEM(tokens.shape, BF16),
            pltpu.VMEM((width // LANES, LANES), BF16),
            pltpu.VMEM(conv_weight.shape, BF16),
            pltpu.VMEM((1, conv_local), F32),
            pltpu.VMEM((1, heads), F32),
            pltpu.VMEM((1, VDIM), F32),
            pltpu.VMEM((rows, heads * VDIM), F32),
            dma((6,)),
            pltpu.SemaphoreType.REGULAR,
            pltpu.SemaphoreType.REGULAR,
        ],
        compiler_params=pltpu.CompilerParams(
            collective_id=0, has_side_effects=True, vmem_limit_bytes=60 * 1024 * 1024
        ),
    )(
        tokens, in_gain.reshape(width // LANES, LANES), w_glu_value, w_glu_gate, w_query, w_key, w_value,
        w_gate_conv, w_gate_attn, conv_weight, conv_gain.reshape(1, conv_local),
        lam.reshape(1, heads),
        head_gain.reshape(1, VDIM), out_conv, out_attn,
    )


def solution(mesh):
    n_sp, n_tp = mesh.shape["sp"], mesh.shape["tp"]
    assert n_tp == 4 and n_sp % 2 == 0 and 2 * QK == VDIM
    col = P(None, "tp")
    in_specs = (
        P("sp", "tp"), P(), col, col, col, col, col, col, col, col,
        P("tp"), P("tp"), P(), P("tp", None), P("tp", None),
    )
    return jax.shard_map(
        functools.partial(local, n_sp, n_tp), mesh=mesh, in_specs=in_specs,
        out_specs=P(("sp", "tp"), None), check_vma=False,
    )
```

```python
import functools
import math

import jax
import jax.numpy as jnp
from jax import lax
from jax.experimental import pallas as pl
from jax.experimental.pallas import tpu as pltpu
from jax.sharding import PartitionSpec as P

EPSILON = 1e-06
NEG_BIG = -1e30
HEAD_SCALE = 0.8
QK = 64
VDIM = 128
MESH = pl.DeviceIdType.MESH
F32 = jnp.float32
BF16 = jnp.bfloat16
PIECES = 3
GATHER = 256
PAD = 32
LANES = 128
CHUNKS = 4
NEAR_STEPS = 3
SKIP = 3
HALF = CHUNKS // 2


def dot(a, b, ca=1, cb=0, precision=None):
    return lax.dot_general(
        a, b, (((ca,), (cb,)), ((), ())), preferred_element_type=F32, precision=precision
    )


def kernel(
    n_sp,
    n_tp,
    tok_hbm,
    gain_hbm,
    w_glu_value,
    w_glu_gate,
    w_query,
    w_key,
    w_value,
    w_gate_conv,
    w_gate_attn,
    taps_hbm,
    conv_gain_hbm,
    lam_hbm,
    head_gain_hbm,
    out_conv,
    out_attn,
    out,
    w_all,
    w_out,
    tokbuf,
    scaled_far,
    acc,
    kv,
    q4,
    m_ref,
    l_ref,
    o_ref,
    gl,
    tail_out,
    tail_in,
    sq_out,
    sq_in,
    ybuf,
    a_out,
    a_own,
    a_in,
    x_out,
    x_in,
    b_out,
    b_own,
    b_in,
    wf,
    yg,
    e_out,
    e_in,
    w_sem,
    tok_send,
    tok_recv,
    kv_recv,
    side_recv,
    up_send,
    skip_send,
    side_send,
    tail_sem,
    sq_send,
    sq_recv,
    a_sem,
    x_sem,
    b_sem,
    g_send,
    g_recv,
    gain32,
    tok,
    gain,
    taps_ref,
    conv_gain,
    lam,
    head_gain,
    ga,
    small_sem,
    near_sem,
    far_sem,
):
    rows, depth = tok.shape
    width = depth * n_tp
    s = lax.axis_index("sp")
    t = lax.axis_index("tp")
    core = t % 2
    p1 = t + 1 - 2 * core
    p2 = (t + 2) % n_tp
    p3 = (p1 + 2) % n_tp
    y = s % 2
    z = s // 2
    nz = n_sp // 2
    mate = s + 1 - 2 * y
    has_up = s + 2 < n_sp
    has_skip = s + 2 * SKIP < n_sp
    size = rows // CHUNKS
    last_static = min(NEAR_STEPS, nz - 1)

    smalls = [
        pltpu.make_async_copy(src, dst, small_sem.at[i])
        for i, (src, dst) in enumerate((
            (tok_hbm, tok), (gain_hbm, gain), (taps_hbm, taps_ref),
            (conv_gain_hbm, conv_gain), (lam_hbm, lam), (head_gain_hbm, head_gain),
        ))
    ]
    for copy in smalls:
        copy.start()
    weights = (w_key, w_value, w_glu_value, w_glu_gate, w_query, w_gate_conv, w_gate_attn)
    spans = []
    at = 0
    loads = []
    for i, w in enumerate(weights):
        cols = w.shape[1]
        spans.append((at, at + cols))
        loads.append(pltpu.make_async_copy(w, w_all.at[:, at : at + cols], w_sem.at[0]))
        at += cols
    at = 0
    out_loads = []
    for i, w in enumerate((out_conv, out_attn)):
        r = w.shape[0]
        out_loads.append(
            pltpu.make_async_copy(w, w_out.at[at : at + r, :], w_sem.at[1])
        )
        at += r

    def tp_copy(src, dst, send, recv, to):
        return pltpu.make_async_remote_copy(
            src_ref=src, dst_ref=dst, send_sem=send, recv_sem=recv,
            device_id={"tp": to}, device_id_type=MESH,
        )

    def sp_copy(src, dst, send, recv, to):
        return pltpu.make_async_remote_copy(
            src_ref=src, dst_ref=dst, send_sem=send, recv_sem=recv,
            device_id={"sp": to}, device_id_type=MESH,
        )

    barrier = pltpu.get_barrier_semaphore()
    for peer in (p1, p2, p3):
        pl.semaphore_signal(barrier, inc=1, device_id={"tp": peer}, device_id_type=MESH)
    expected = jnp.int32(3)
    for by in (1, 2):
        for other in (s - by, s + by):
            valid = (other >= 0) & (other < n_sp)
            expected = expected + valid.astype(jnp.int32)

            @pl.when(valid)
            def _():
                pl.semaphore_signal(barrier, inc=1, device_id={"sp": other}, device_id_type=MESH)

    for copy in smalls:
        copy.wait()
    for copy in loads:
        copy.start()
    pl.semaphore_wait(barrier, expected)

    def piece_rows(q):
        return slice(q * size, (q + 1) * size)

    across = [
        tp_copy(
            tok.at[piece_rows(q)], tokbuf.at[1, piece_rows(q)],
            tok_send.at[0], tok_recv.at[q], p3,
        )
        for q in range(CHUNKS)
    ]
    passed = [
        tp_copy(
            tokbuf.at[1, piece_rows(q)], tokbuf.at[2, piece_rows(q)],
            tok_send.at[1], tok_recv.at[CHUNKS + q], p1,
        )
        for q in range(CHUNKS)
    ]
    beside = tp_copy(tok, tokbuf.at[0], tok_send.at[2], tok_recv.at[2 * CHUNKS], p1)
    across[0].start()
    beside.start()

    @pl.when(core == 0)
    def _():
        for copy in across[1:]:
            copy.start()

    for copy in out_loads:
        copy.start()

    def tell(sem):
        pl.semaphore_signal(sem, inc=1, device_id={"sp": s - 2}, device_id_type=MESH)

    @pl.when((s >= 2) & has_up)
    def _():
        tell(near_sem)

    def sent(ref, sem):
        pltpu.make_async_copy(ref, ref, sem).wait()

    lines = depth // LANES

    def prepare(x, owner):
        wide = x.astype(F32)
        parts = [
            wide[:, b * LANES : (b + 1) * LANES] * gain32[pl.ds(owner * lines + b, 1), :]
            for b in range(lines)
        ]
        scaled = jnp.concatenate(parts, axis=1).astype(BF16)
        return scaled, jnp.sum(wide * wide, axis=1, keepdims=True)

    def w_rows(owner, lo, hi):
        return w_all[pl.ds(pl.multiple_of(owner * depth, depth), depth), lo:hi]

    first_cols = spans[3][1]
    total_cols = spans[-1][1]
    gain32[...] = gain[...].astype(F32)
    scaled_own, squares = prepare(tok[...], t)
    @pl.when(s + 4 < n_sp)
    def _():
        pl.semaphore_wait(near_sem, 1)

    @pl.when((s >= 2) & (s + 4 < n_sp))
    def _():
        tell(far_sem)

    pltpu.make_async_copy(w_all, w_all, w_sem.at[0]).wait()

    @pl.when(core == 1)
    def _():
        for copy in across[1:]:
            copy.start()

    beside.wait_recv()
    scaled, more = prepare(tokbuf[0], p1)
    squares = squares + more
    acc[...] = dot(
        jnp.concatenate([scaled_own, scaled], axis=1),
        jnp.concatenate([w_rows(t, 0, total_cols), w_rows(p1, 0, total_cols)], axis=0),
    )

    def late(q):
        at = piece_rows(q)
        lhs = jnp.concatenate([scaled_far[0, at], scaled_far[1, at]], axis=1)
        rhs = jnp.concatenate(
            [w_rows(p3, first_cols, total_cols), w_rows(p2, first_cols, total_cols)], axis=0
        )
        acc[at, first_cols:] += dot(lhs, rhs)

    def chunk(j, q):
        return kv.at[j, :, piece_rows(q), :]

    def up(j, q):
        return sp_copy(chunk(j, q), chunk(j, q), up_send.at[j // 2], kv_recv.at[j // 2, q], s + 2)

    def skip(q):
        return sp_copy(chunk(s, q), chunk(s, q), skip_send.at[0], kv_recv.at[z, q], s + 2 * SKIP)

    def side(j, q):
        return sp_copy(chunk(j, q), chunk(j, q), side_send.at[j // 2], side_recv.at[j // 2, q // HALF], mate)

    def relay(k, q):
        j = s - 2 * k
        up(j, q).wait_recv()
        if isinstance(k, int):
            if k != SKIP - 1:

                @pl.when(has_up)
                def _():
                    up(j, q).start()
        else:

            @pl.when(has_up & (k != SKIP - 1))
            def _():
                up(j, q).start()

        side(j, q).start()

    def due(steps, k, q):
        if k == 1:
            return 9.9 + 1.43 * q
        return 11.3 + 1.3 * q if k == SKIP else 14.9 + 0.7 * q

    pending = {
        steps: sorted(
            ((k, q) for k in range(1, steps + 1) for q in range(CHUNKS)),
            key=lambda e: due(steps, *e),
        )
        for steps in range(1, last_static + 1)
    }

    for queue in pending.values():
        queue.remove((1, 0))

    def relays(until):
        for steps, queue in pending.items():
            now = []
            while queue and due(steps, *queue[0]) < until:
                now.append(queue.pop(0))
            if not now:
                continue

            @pl.when((z == steps) if steps < last_static else (z >= steps))
            def _():
                for k, q in now:
                    relay(k, q)

    tail = sp_copy(tail_out, tail_in, tail_sem.at[0], tail_sem.at[1], s + 1)
    inv_parts = []
    for q in range(CHUNKS):
        at = piece_rows(q)
        across[q].wait_recv()
        passed[q].start()
        scaled, sq2 = prepare(tokbuf[1, at], p3)
        scaled_far[0, at] = scaled
        part = acc[at, :first_cols] + dot(scaled, w_rows(p3, 0, first_cols))
        if q > 0:
            late(q - 1)
        passed[q].wait_recv()
        scaled, sq3 = prepare(tokbuf[2, at], p2)
        scaled_far[1, at] = scaled
        part = part + dot(scaled, w_rows(p2, 0, first_cols))
        inv = lax.rsqrt((squares[at] + sq2 + sq3) / width + EPSILON)
        inv_parts.append(inv)
        part = (part * inv).astype(BF16)

        def glue():
            value = part[:, spans[2][0] : spans[2][1]].astype(F32)
            gate = part[:, spans[3][0] : spans[3][1]].astype(F32)
            glued = (value * jax.nn.sigmoid(gate)).astype(BF16)
            gl[PAD + q * size : PAD + (q + 1) * size, :] = glued.astype(F32)
            return glued

        if q == CHUNKS - 1:
            tail_out[...] = glue()[size - PAD :]

            @pl.when(s + 1 < n_sp)
            def _():
                tail.start()

        kv[s, 0, at] = part[:, : spans[0][1]]
        kv[s, 1, at] = part[:, spans[1][0] : spans[1][1]]

        @pl.when(y == 0)
        def _():
            side(s, q).start()

        @pl.when(has_up)
        def _():
            up(s, q).start()

        @pl.when(has_skip)
        def _():
            if q == 0:
                pl.semaphore_wait(far_sem, 1)
            skip(q).start()

        if q < CHUNKS - 1:
            glue()
        if q == CHUNKS - 2:

            @pl.when((z >= 1) & (core == 1))
            def _():
                relay(1, 0)

        if q == CHUNKS - 1:

            @pl.when((z >= 1) & (core == 0))
            def _():
                relay(1, 0)

        relays(7.2 + 1.4 * q)
    late(CHUNKS - 1)
    sent(w_out, w_sem.at[1])
    shared = w_out.shape[1] - 2 * GATHER

    def gather_cols(parity):
        return pl.ds(pl.multiple_of(shared + parity * GATHER, GATHER), GATHER)

    w_copies = [
        tp_copy(w_out.at[:, gather_cols(parity)], wf.at[i], g_send.at[i], g_recv.at[i], p)
        for i, (p, parity) in enumerate(((p1, 1 - core), (p2, core), (p3, 1 - core)))
    ]
    w_copies[0].start()
    w_copies[1].start()
    inv_rms = jnp.concatenate(inv_parts, axis=0)

    def projected(i, lo=0, hi=None):
        hi = rows if hi is None else hi
        a, b = spans[i]
        return (acc[lo:hi, a:b] * inv_rms[lo:hi]).astype(BF16)

    query = projected(4).astype(F32) * (1.0 / math.sqrt(QK))
    heads = w_query.shape[1] // (2 * QK)
    maps = 2 * heads
    lane = lax.broadcasted_iota(jnp.int32, (rows, 2 * QK), 1)
    for h in range(heads):
        qh = query[:, h * 2 * QK : (h + 1) * 2 * QK]
        for m in range(2):
            keep = (lane >= m * QK) & (lane < (m + 1) * QK)
            q4[2 * h + m] = jnp.where(keep, qh, 0.0).astype(BF16)
    relays(11.9)

    key_pos = lax.broadcasted_iota(jnp.int32, (rows, rows), 0)
    query_pos = lax.broadcasted_iota(jnp.int32, (rows, rows), 1)
    allowed = key_pos <= query_pos
    k_own = kv[s, 0]
    v_own = kv[s, 1]
    scores = [jnp.where(allowed, dot(k_own, q4[i], 1, 1), NEG_BIG) for i in range(maps)]
    tops = [jnp.max(x, axis=0, keepdims=True) for x in scores]
    exps = [jnp.exp(x - top) for x, top in zip(scores, tops)]
    for i in range(maps):
        m_ref[i] = tops[i]
        l_ref[i] = jnp.sum(exps[i], axis=0, keepdims=True)
        o_ref[i] = dot(v_own, exps[i].astype(BF16), 0, 0)
    relays(12.8)

    gate_attn = projected(6).astype(F32)
    ga[...] = gate_attn * jax.nn.sigmoid(gate_attn)

    def visit(blocks, at=slice(None)):
        def stacked(plane):
            parts = [
                kv[b[0], plane, b[1] : b[2]] if isinstance(b, tuple) else kv[b, plane]
                for b in blocks
            ]
            return parts[0] if len(parts) == 1 else jnp.concatenate(parts, axis=0)

        k = stacked(0)
        v = stacked(1)
        scores = [dot(k, q4[i, at, :], 1, 1) for i in range(maps)]
        olds = [m_ref[i, :, at] for i in range(maps)]
        tops = [
            jnp.maximum(old, jnp.max(x, axis=0, keepdims=True)) for old, x in zip(olds, scores)
        ]
        exps = [jnp.exp(x - top) for x, top in zip(scores, tops)]
        factors = [jnp.exp(old - top) for old, top in zip(olds, tops)]
        news = [dot(v, e.astype(BF16), 0, 0) for e in exps]
        for i in range(maps):
            m_ref[i, :, at] = tops[i]
            l_ref[i, :, at] = l_ref[i, :, at] * factors[i] + jnp.sum(exps[i], axis=0, keepdims=True)
            o_ref[i, :, at] = o_ref[i, :, at] * factors[i] + news[i]

    middle = rows // 2

    def mate_arrives(k, halves=(0, 1)):
        for half in halves:
            ref = kv.at[mate - 2 * k, :, half * middle : (half + 1) * middle, :]
            sent(ref, side_recv.at[z - k, half])

    sq_copies = [
        tp_copy(sq_out, sq_in.at[i], sq_send.at[0], sq_recv.at[i], p)
        for i, p in enumerate((p1, p2, p3))
    ]
    high = lax.Precision.HIGHEST

    def convolve():
        @pl.when(s == 0)
        def _():
            gl[:PAD, :] = jnp.zeros((PAD, gl.shape[1]), F32)

        @pl.when(s > 0)
        def _():
            tail.wait_recv()
            gl[:PAD, :] = tail_in[...].astype(F32)

        n_taps = taps_ref.shape[0]
        taps = taps_ref[...].astype(F32)
        conv = jnp.zeros((rows, gl.shape[1]), F32)
        for j in range(n_taps):
            lo = PAD - (n_taps - 1) + j
            conv = conv + gl[lo : lo + rows, :] * taps[j : j + 1, :]
        ones = jnp.ones((8, conv.shape[1]), F32)
        sq_out[...] = dot(ones, conv * conv, 1, 1, high)
        gl[PAD:, :] = conv
        for copy in sq_copies:
            copy.start()
        w_copies[2].start()
    @pl.when(y == 1)
    def _():
        convolve()

    relays(14.01)

    relays(15.25)

    @pl.when(z >= 1)
    def _():
        visit([s - 2])

    relays(15.65)

    @pl.when(y == 0)
    def _():
        convolve()

    relays(16.6)

    @pl.when(y == 1)
    def _():
        mate_arrives(0)

    @pl.when((y == 1) & (z > 0))
    def _():
        visit([mate])

    conv_local = gl.shape[1]
    relays(100.0)

    if last_static >= 2:

        @pl.when(z == 2)
        def _():
            visit([s - 4])

    if last_static >= 3:

        @pl.when(z >= 3)
        def _():
            visit([s - 4, s - 6])

    def beyond(k, carry):
        for q in range(CHUNKS):
            relay(k, q)
        visit([s - 2 * k])
        return carry

    if nz - 1 > NEAR_STEPS:
        lax.fori_loop(NEAR_STEPS + 1, z + 1, beyond, 0)

    conv_local = gl.shape[1]
    gate_conv = projected(5).astype(F32)
    for copy in sq_copies:
        copy.wait_recv()
    total_sq = sq_out[...] + sq_in[0] + sq_in[1] + sq_in[2]
    spread = jnp.full((8, conv_local), 0.125, F32)
    mean_sq = dot(total_sq, spread, 0, 0, high) / (conv_local * n_tp)
    normed = gl[PAD:, :] * lax.rsqrt(mean_sq + EPSILON) * conv_gain[...]
    ybuf[:, :conv_local] = (
        normed * jax.nn.sigmoid(normed) * (gate_conv * jax.nn.sigmoid(gate_conv))
    ).astype(BF16)

    part = rows // n_tp
    both = 2 * part
    far_rows = pl.ds(pl.multiple_of(p2 // 2 * both, both), both)
    near_rows = pl.ds(pl.multiple_of(t // 2 * both, both), both)
    yc_copy = tp_copy(
        ybuf.at[far_rows, :conv_local], yg.at[1, :, :conv_local], g_send.at[3], g_recv.at[3], p3
    )
    ya_copy = tp_copy(
        ybuf.at[far_rows, conv_local:], yg.at[1, :, conv_local:], g_send.at[4], g_recv.at[4], p3
    )
    yc_copy.start()

    def finish(at):
        for h in range(heads):
            first_map = o_ref[2 * h, :, at] / l_ref[2 * h, :, at]
            second_map = o_ref[2 * h + 1, :, at] / l_ref[2 * h + 1, :, at]
            o = first_map - lam[:, h : h + 1] * second_map
            n = o * lax.rsqrt(jnp.mean(o * o, axis=0, keepdims=True) + EPSILON)
            n = jnp.transpose(n) * head_gain[...] * HEAD_SCALE
            lo = h * VDIM
            ybuf[at, conv_local + lo : conv_local + lo + VDIM] = (
                n * ga[at, lo : lo + VDIM]
            ).astype(BF16)

    def beyond_mate(k, carry):
        mate_arrives(k)
        visit([mate - 2 * k])
        return carry

    if nz - 1 > NEAR_STEPS:
        lax.fori_loop(NEAR_STEPS + 1, z + 1, beyond_mate, 0)

    @pl.when(z >= 1)
    def _():
        mate_arrives(1)

    if last_static >= 2:

        @pl.when(z >= 2)
        def _():
            visit([mate - 2])

    if last_static >= 3:

        @pl.when(z >= 3)
        def _():
            mate_arrives(3)
            visit([mate - 6])

    if last_static >= 2:

        @pl.when(z >= 2)
        def _():
            mate_arrives(2, (0,))
            visit([(mate - 4, 0, middle)])
            mate_arrives(2, (1,))

    def last_mate(at):
        @pl.when((z == 0) & (y == 1))
        def _():
            visit([mate], at)

        @pl.when(z == 1)
        def _():
            visit([mate - 2], at)

        if last_static >= 2:

            @pl.when(z >= 2)
            def _():
                visit([(mate - 4, middle, rows)], at)

    last_mate(far_rows)
    finish(far_rows)

    def block(p):
        return ybuf[pl.ds(pl.multiple_of(p * part, part), part), :]

    ya_copy.start()
    lanes = shared // LANES
    edges = [LANES * (lanes * c // PIECES) for c in range(PIECES + 1)]
    ranges = [slice(lo, hi) for lo, hi in zip(edges, edges[1:])]
    far = jnp.concatenate([block(p2), block(p3)], axis=0)
    a_copies = []
    for c, at in enumerate(ranges):
        r = dot(far, w_out[:, at]).astype(BF16)
        a_out[:, at] = r[:part]
        a_own[:, at] = r[part:]
        copy = tp_copy(a_out.at[:, at], a_in.at[:, at], a_sem.at[0], a_sem.at[1 + c], p1)
        copy.start()
        a_copies.append(copy)
    x_copies = []
    for c, at in enumerate(ranges):
        a_copies[c].wait_recv()
        x_out[:, at] = (a_own[:, at].astype(F32) + a_in[:, at].astype(F32)).astype(BF16)
        copy = tp_copy(x_out.at[:, at], x_in.at[:, at], x_sem.at[0], x_sem.at[1 + c], p3)
        copy.start()
        x_copies.append(copy)
    last_mate(near_rows)
    finish(near_rows)
    yn_copy = tp_copy(ybuf.at[near_rows, :], yg.at[0], g_send.at[5], g_recv.at[5], p1)
    yn_copy.start()
    near = jnp.concatenate([block(p1), block(t)], axis=0)
    for c in range(2):
        at = slice(c * (shared // 2), (c + 1) * (shared // 2))
        r = dot(near, w_out[:, at]).astype(BF16)
        b_out[:, at] = r[:part]
        b_own[:, at] = r[part:].astype(F32)
    b_copy = tp_copy(b_out, b_in, b_sem.at[0], b_sem.at[1], p1)
    b_copy.start()
    yc_copy.wait_recv()
    ya_copy.wait_recv()
    pass_copy = tp_copy(yg.at[1], yg.at[2], g_send.at[6], g_recv.at[6], p1)
    pass_copy.start()
    for copy in w_copies:
        copy.wait_recv()
    yn_copy.wait_recv()
    whole = dot(ybuf[near_rows, :], w_out[:, gather_cols(core)])
    whole = whole + dot(yg[0], wf[0]) + dot(yg[1], wf[2])
    pass_copy.wait_recv()
    e_out[...] = (whole + dot(yg[2], wf[1])).astype(BF16)
    e_copy = tp_copy(
        e_out.at[pl.ds(pl.multiple_of((1 - core) * part, part), part)], e_in,
        g_send.at[7], g_recv.at[7], p1,
    )
    e_copy.start()
    sent(tok, tok_send.at[0])
    sent(tok, tok_send.at[1])
    sent(tok, tok_send.at[2])
    sent(sq_in, sq_send.at[0])
    sent(a_out, a_sem.at[0])

    @pl.when(s + 1 < n_sp)
    def _():
        tail.wait_send()

    @pl.when(has_up)
    def _():
        sent(kv.at[s], up_send.at[z])

    @pl.when(has_skip)
    def _():
        sent(kv.at[s], skip_send.at[0])

    @pl.when(y == 0)
    def _():
        sent(kv.at[s], side_send.at[z])

    def drain(k, carry):
        j = s - 2 * k

        @pl.when(has_up & (k != SKIP - 1))
        def _():
            sent(kv.at[j], up_send.at[z - k])

        sent(kv.at[j], side_send.at[z - k])
        return carry

    lax.fori_loop(1, z + 1, drain, 0)
    b_copy.wait_recv()
    b_own[...] = b_own[...] + b_in[...].astype(F32)
    e_copy.wait_recv()
    out[:, gather_cols(core)] = e_out[pl.ds(pl.multiple_of(core * part, part), part), :]
    out[:, gather_cols(1 - core)] = e_in[...]
    for copy in w_copies + [yc_copy, ya_copy, yn_copy, pass_copy, e_copy]:
        copy.wait_send()
    for c, at in enumerate(ranges):
        x_copies[c].wait_recv()
        out[:, at] = (b_own[:, at] + x_in[:, at].astype(F32)).astype(BF16)
    sent(x_out, x_sem.at[0])
    sent(b_out, b_sem.at[0])


def local(n_sp, n_tp, *args):
    (tokens, in_gain, w_glu_value, w_glu_gate, w_query, w_key, w_value, w_gate_conv,
     w_gate_attn, conv_weight, conv_gain, lam, head_gain, out_conv, out_attn) = args
    rows, depth = tokens.shape
    width = depth * n_tp
    weights = (w_glu_value, w_glu_gate, w_query, w_key, w_value, w_gate_conv, w_gate_attn)
    total_cols = sum(w.shape[1] for w in weights)
    out_rows = out_conv.shape[0] + out_attn.shape[0]
    out_cols = out_conv.shape[1]
    conv_local = conv_weight.shape[1]
    heads = lam.shape[0]
    part = rows // n_tp
    vmem = pl.BlockSpec(memory_space=pltpu.VMEM)
    hbm = pl.BlockSpec(memory_space=pl.ANY)
    dma = pltpu.SemaphoreType.DMA
    shared = out_cols - 2 * GATHER
    piece = pltpu.VMEM((part, shared), BF16)
    return pl.pallas_call(
        functools.partial(kernel, n_sp, n_tp),
        out_shape=pltpu.VMEM((part, out_cols), BF16),
        in_specs=[hbm] * len(args),
        out_specs=vmem,
        scratch_shapes=[
            pltpu.VMEM((width, total_cols), BF16),
            pltpu.VMEM((out_rows, out_cols), BF16),
            pltpu.VMEM((3, rows, depth), BF16),
            pltpu.VMEM((2, rows, depth), BF16),
            pltpu.VMEM((rows, total_cols), F32),
            pltpu.VMEM((n_sp, 2, rows, VDIM), BF16),
            pltpu.VMEM((2 * heads, rows, 2 * QK), BF16),
            pltpu.VMEM((2 * heads, 1, rows), F32),
            pltpu.VMEM((2 * heads, 1, rows), F32),
            pltpu.VMEM((2 * heads, VDIM, rows), F32),
            pltpu.VMEM((PAD + rows, conv_local), F32),
            pltpu.VMEM((PAD, conv_local), BF16),
            pltpu.VMEM((PAD, conv_local), BF16),
            pltpu.VMEM((8, rows), F32),
            pltpu.VMEM((3, 8, rows), F32),
            pltpu.VMEM((rows, out_rows), BF16),
            piece, piece, piece, piece, piece, piece,
            pltpu.VMEM((part, shared), F32),
            piece,
            pltpu.VMEM((3, out_rows, GATHER), BF16),
            pltpu.VMEM((3, 2 * part, out_rows), BF16),
            pltpu.VMEM((2 * part, GATHER), BF16),
            pltpu.VMEM((part, GATHER), BF16),
            dma((2,)),
            dma((3,)),
            dma((2 * CHUNKS + 1,)),
            dma((max(n_sp // 2 - 1, 1), CHUNKS)),
            dma((n_sp // 2, 2)),
            dma((n_sp // 2,)),
            dma((1,)),
            dma((n_sp // 2,)),
            dma((2,)),
            dma((1,)),
            dma((3,)),
            dma((1 + PIECES,)),
            dma((1 + PIECES,)),
            dma((2,)),
            dma((8,)),
            dma((8,)),
            pltpu.VMEM((width // LANES, LANES), F32),
            pltpu.VMEM(tokens.shape, BF16),
            pltpu.VMEM((width // LANES, LANES), BF16),
            pltpu.VMEM(conv_weight.shape, BF16),
            pltpu.VMEM((1, conv_local), F32),
            pltpu.VMEM((1, heads), F32),
            pltpu.VMEM((1, VDIM), F32),
            pltpu.VMEM((rows, heads * VDIM), F32),
            dma((6,)),
            pltpu.SemaphoreType.REGULAR,
            pltpu.SemaphoreType.REGULAR,
        ],
        compiler_params=pltpu.CompilerParams(
            collective_id=0, has_side_effects=True, vmem_limit_bytes=60 * 1024 * 1024
        ),
    )(
        tokens, in_gain.reshape(width // LANES, LANES), w_glu_value, w_glu_gate, w_query, w_key, w_value,
        w_gate_conv, w_gate_attn, conv_weight, conv_gain.reshape(1, conv_local),
        lam.reshape(1, heads),
        head_gain.reshape(1, VDIM), out_conv, out_attn,
    )


def solution(mesh):
    n_sp, n_tp = mesh.shape["sp"], mesh.shape["tp"]
    assert n_tp == 4 and n_sp % 2 == 0 and 2 * QK == VDIM
    col = P(None, "tp")
    in_specs = (
        P("sp", "tp"), P(), col, col, col, col, col, col, col, col,
        P("tp"), P("tp"), P(), P("tp", None), P("tp", None),
    )
    return jax.shard_map(
        functools.partial(local, n_sp, n_tp), mesh=mesh, in_specs=in_specs,
        out_specs=P(("sp", "tp"), None), check_vma=False,
    )
```

```python
import functools
import math

import jax
import jax.numpy as jnp
from jax import lax
from jax.experimental import pallas as pl
from jax.experimental.pallas import tpu as pltpu
from jax.sharding import PartitionSpec as P

EPSILON = 1e-06
NEG_BIG = -1e30
HEAD_SCALE = 0.8
QK = 64
VDIM = 128
MESH = pl.DeviceIdType.MESH
F32 = jnp.float32
BF16 = jnp.bfloat16
PIECES = 3
GATHER = 256
PAD = 32
LANES = 128
CHUNKS = 4
NEAR_STEPS = 3
SKIP = 3
HALF = CHUNKS // 2


def dot(a, b, ca=1, cb=0, precision=None):
    return lax.dot_general(
        a, b, (((ca,), (cb,)), ((), ())), preferred_element_type=F32, precision=precision
    )


def kernel(
    n_sp,
    n_tp,
    tok_hbm,
    gain_hbm,
    w_glu_value,
    w_glu_gate,
    w_query,
    w_key,
    w_value,
    w_gate_conv,
    w_gate_attn,
    taps_hbm,
    conv_gain_hbm,
    lam_hbm,
    head_gain_hbm,
    out_conv,
    out_attn,
    out,
    w_all,
    w_out,
    tokbuf,
    scaled_far,
    acc,
    kv,
    q4,
    m_ref,
    l_ref,
    o_ref,
    gl,
    tail_out,
    tail_in,
    sq_out,
    sq_in,
    ybuf,
    a_out,
    a_own,
    a_in,
    x_out,
    x_in,
    b_out,
    b_own,
    b_in,
    wf,
    yg,
    e_out,
    e_in,
    w_sem,
    tok_send,
    tok_recv,
    kv_recv,
    side_recv,
    up_send,
    skip_send,
    side_send,
    tail_sem,
    sq_send,
    sq_recv,
    a_sem,
    x_sem,
    b_sem,
    g_send,
    g_recv,
    gain32,
    tok,
    gain,
    taps_ref,
    conv_gain,
    lam,
    head_gain,
    ga,
    small_sem,
    near_sem,
    far_sem,
):
    rows, depth = tok.shape
    width = depth * n_tp
    s = lax.axis_index("sp")
    t = lax.axis_index("tp")
    core = t % 2
    p1 = t + 1 - 2 * core
    p2 = (t + 2) % n_tp
    p3 = (p1 + 2) % n_tp
    y = s % 2
    z = s // 2
    nz = n_sp // 2
    mate = s + 1 - 2 * y
    has_up = s + 2 < n_sp
    has_skip = s + 2 * SKIP < n_sp
    size = rows // CHUNKS
    last_static = min(NEAR_STEPS, nz - 1)

    smalls = [
        pltpu.make_async_copy(src, dst, small_sem.at[i])
        for i, (src, dst) in enumerate((
            (tok_hbm, tok), (gain_hbm, gain), (taps_hbm, taps_ref),
            (conv_gain_hbm, conv_gain), (lam_hbm, lam), (head_gain_hbm, head_gain),
        ))
    ]
    for copy in smalls:
        copy.start()
    weights = (w_key, w_value, w_glu_value, w_glu_gate, w_query, w_gate_conv, w_gate_attn)
    spans = []
    at = 0
    loads = []
    for i, w in enumerate(weights):
        cols = w.shape[1]
        spans.append((at, at + cols))
        loads.append(pltpu.make_async_copy(w, w_all.at[:, at : at + cols], w_sem.at[0]))
        at += cols
    at = 0
    out_loads = []
    for i, w in enumerate((out_conv, out_attn)):
        r = w.shape[0]
        out_loads.append(
            pltpu.make_async_copy(w, w_out.at[at : at + r, :], w_sem.at[1])
        )
        at += r

    def tp_copy(src, dst, send, recv, to):
        return pltpu.make_async_remote_copy(
            src_ref=src, dst_ref=dst, send_sem=send, recv_sem=recv,
            device_id={"tp": to}, device_id_type=MESH,
        )

    def sp_copy(src, dst, send, recv, to):
        return pltpu.make_async_remote_copy(
            src_ref=src, dst_ref=dst, send_sem=send, recv_sem=recv,
            device_id={"sp": to}, device_id_type=MESH,
        )

    barrier = pltpu.get_barrier_semaphore()
    for peer in (p1, p2, p3):
        pl.semaphore_signal(barrier, inc=1, device_id={"tp": peer}, device_id_type=MESH)
    expected = jnp.int32(3)
    for by in (1, 2):
        for other in (s - by, s + by):
            valid = (other >= 0) & (other < n_sp)
            expected = expected + valid.astype(jnp.int32)

            @pl.when(valid)
            def _():
                pl.semaphore_signal(barrier, inc=1, device_id={"sp": other}, device_id_type=MESH)

    for copy in smalls:
        copy.wait()
    for copy in loads:
        copy.start()
    pl.semaphore_wait(barrier, expected)

    def piece_rows(q):
        return slice(q * size, (q + 1) * size)

    across = [
        tp_copy(
            tok.at[piece_rows(q)], tokbuf.at[1, piece_rows(q)],
            tok_send.at[0], tok_recv.at[q], p3,
        )
        for q in range(CHUNKS)
    ]
    passed = [
        tp_copy(
            tokbuf.at[1, piece_rows(q)], tokbuf.at[2, piece_rows(q)],
            tok_send.at[0], tok_recv.at[CHUNKS + q], p1,
        )
        for q in range(CHUNKS)
    ]
    beside = tp_copy(tok, tokbuf.at[0], tok_send.at[0], tok_recv.at[2 * CHUNKS], p1)
    across[0].start()
    beside.start()

    @pl.when(core == 0)
    def _():
        for copy in across[1:]:
            copy.start()

    for copy in out_loads:
        copy.start()

    def tell(sem):
        pl.semaphore_signal(sem, inc=1, device_id={"sp": s - 2}, device_id_type=MESH)

    @pl.when((s >= 2) & has_up)
    def _():
        tell(near_sem)

    def sent(ref, sem):
        pltpu.make_async_copy(ref, ref, sem).wait()

    lines = depth // LANES

    def prepare(x, owner):
        wide = x.astype(F32)
        parts = [
            wide[:, b * LANES : (b + 1) * LANES] * gain32[pl.ds(owner * lines + b, 1), :]
            for b in range(lines)
        ]
        scaled = jnp.concatenate(parts, axis=1).astype(BF16)
        return scaled, jnp.sum(wide * wide, axis=1, keepdims=True)

    def w_rows(owner, lo, hi):
        return w_all[pl.ds(pl.multiple_of(owner * depth, depth), depth), lo:hi]

    first_cols = spans[3][1]
    total_cols = spans[-1][1]
    gain32[...] = gain[...].astype(F32)
    scaled_own, squares = prepare(tok[...], t)
    @pl.when(s + 4 < n_sp)
    def _():
        pl.semaphore_wait(near_sem, 1)

    @pl.when((s >= 2) & (s + 4 < n_sp))
    def _():
        tell(far_sem)

    pltpu.make_async_copy(w_all, w_all, w_sem.at[0]).wait()

    @pl.when(core == 1)
    def _():
        for copy in across[1:]:
            copy.start()

    beside.wait_recv()
    scaled, more = prepare(tokbuf[0], p1)
    squares = squares + more
    acc[...] = dot(
        jnp.concatenate([scaled_own, scaled], axis=1),
        jnp.concatenate([w_rows(t, 0, total_cols), w_rows(p1, 0, total_cols)], axis=0),
    )

    def late(q):
        at = piece_rows(q)
        lhs = jnp.concatenate([scaled_far[0, at], scaled_far[1, at]], axis=1)
        rhs = jnp.concatenate(
            [w_rows(p3, first_cols, total_cols), w_rows(p2, first_cols, total_cols)], axis=0
        )
        acc[at, first_cols:] += dot(lhs, rhs)

    def chunk(j, q):
        return kv.at[j, :, piece_rows(q), :]

    def up(j, q):
        return sp_copy(chunk(j, q), chunk(j, q), up_send.at[j // 2], kv_recv.at[j // 2, q], s + 2)

    def skip(q):
        return sp_copy(chunk(s, q), chunk(s, q), skip_send.at[0], kv_recv.at[z, q], s + 2 * SKIP)

    def side(j, q):
        return sp_copy(chunk(j, q), chunk(j, q), side_send.at[j // 2], side_recv.at[j // 2, q // HALF], mate)

    def relay(k, q):
        j = s - 2 * k
        up(j, q).wait_recv()
        if isinstance(k, int):
            if k != SKIP - 1:

                @pl.when(has_up)
                def _():
                    up(j, q).start()
        else:

            @pl.when(has_up & (k != SKIP - 1))
            def _():
                up(j, q).start()

        side(j, q).start()

    def due(steps, k, q):
        if k == 1:
            return 9.9 + 1.43 * q
        return 11.3 + 1.3 * q if k == SKIP else 14.9 + 0.7 * q

    pending = {
        steps: sorted(
            ((k, q) for k in range(1, steps + 1) for q in range(CHUNKS)),
            key=lambda e: due(steps, *e),
        )
        for steps in range(1, last_static + 1)
    }

    for queue in pending.values():
        queue.remove((1, 0))

    def relays(until):
        for steps, queue in pending.items():
            now = []
            while queue and due(steps, *queue[0]) < until:
                now.append(queue.pop(0))
            if not now:
                continue

            @pl.when((z == steps) if steps < last_static else (z >= steps))
            def _():
                for k, q in now:
                    relay(k, q)

    tail = sp_copy(tail_out, tail_in, tail_sem.at[0], tail_sem.at[1], s + 1)
    inv_parts = []
    for q in range(CHUNKS):
        at = piece_rows(q)
        across[q].wait_recv()
        passed[q].start()
        scaled, sq2 = prepare(tokbuf[1, at], p3)
        scaled_far[0, at] = scaled
        part = acc[at, :first_cols] + dot(scaled, w_rows(p3, 0, first_cols))
        if q > 0:
            late(q - 1)
        passed[q].wait_recv()
        scaled, sq3 = prepare(tokbuf[2, at], p2)
        scaled_far[1, at] = scaled
        part = part + dot(scaled, w_rows(p2, 0, first_cols))
        inv = lax.rsqrt((squares[at] + sq2 + sq3) / width + EPSILON)
        inv_parts.append(inv)
        part = (part * inv).astype(BF16)

        def glue():
            value = part[:, spans[2][0] : spans[2][1]].astype(F32)
            gate = part[:, spans[3][0] : spans[3][1]].astype(F32)
            glued = (value * jax.nn.sigmoid(gate)).astype(BF16)
            gl[PAD + q * size : PAD + (q + 1) * size, :] = glued.astype(F32)
            return glued

        if q == CHUNKS - 1:
            tail_out[...] = glue()[size - PAD :]

            @pl.when(s + 1 < n_sp)
            def _():
                tail.start()

        kv[s, 0, at] = part[:, : spans[0][1]]
        kv[s, 1, at] = part[:, spans[1][0] : spans[1][1]]

        @pl.when(y == 0)
        def _():
            side(s, q).start()

        @pl.when(has_up)
        def _():
            up(s, q).start()

        @pl.when(has_skip)
        def _():
            if q == 0:
                pl.semaphore_wait(far_sem, 1)
            skip(q).start()

        if q < CHUNKS - 1:
            glue()
        if q == CHUNKS - 2:

            @pl.when((z >= 1) & (core == 1))
            def _():
                relay(1, 0)

        if q == CHUNKS - 1:

            @pl.when((z >= 1) & (core == 0))
            def _():
                relay(1, 0)

        relays(7.2 + 1.4 * q)
    late(CHUNKS - 1)
    sent(w_out, w_sem.at[1])
    shared = w_out.shape[1] - 2 * GATHER

    def gather_cols(parity):
        return pl.ds(pl.multiple_of(shared + parity * GATHER, GATHER), GATHER)

    w_copies = [
        tp_copy(w_out.at[:, gather_cols(parity)], wf.at[i], g_send.at[0], g_recv.at[0], p)
        for i, (p, parity) in enumerate(((p1, 1 - core), (p2, core), (p3, 1 - core)))
    ]
    w_copies[0].start()
    w_copies[1].start()
    inv_rms = jnp.concatenate(inv_parts, axis=0)

    def projected(i, lo=0, hi=None):
        hi = rows if hi is None else hi
        a, b = spans[i]
        return (acc[lo:hi, a:b] * inv_rms[lo:hi]).astype(BF16)

    query = projected(4).astype(F32) * (1.0 / math.sqrt(QK))
    heads = w_query.shape[1] // (2 * QK)
    maps = 2 * heads
    lane = lax.broadcasted_iota(jnp.int32, (rows, 2 * QK), 1)
    for h in range(heads):
        qh = query[:, h * 2 * QK : (h + 1) * 2 * QK]
        for m in range(2):
            keep = (lane >= m * QK) & (lane < (m + 1) * QK)
            q4[2 * h + m] = jnp.where(keep, qh, 0.0).astype(BF16)
    relays(11.9)

    key_pos = lax.broadcasted_iota(jnp.int32, (rows, rows), 0)
    query_pos = lax.broadcasted_iota(jnp.int32, (rows, rows), 1)
    allowed = key_pos <= query_pos
    k_own = kv[s, 0]
    v_own = kv[s, 1]
    scores = [jnp.where(allowed, dot(k_own, q4[i], 1, 1), NEG_BIG) for i in range(maps)]
    tops = [jnp.max(x, axis=0, keepdims=True) for x in scores]
    exps = [jnp.exp(x - top) for x, top in zip(scores, tops)]
    for i in range(maps):
        m_ref[i] = tops[i]
        l_ref[i] = jnp.sum(exps[i], axis=0, keepdims=True)
        o_ref[i] = dot(v_own, exps[i].astype(BF16), 0, 0)
    relays(12.8)

    gate_attn = projected(6).astype(F32)
    ga[...] = gate_attn * jax.nn.sigmoid(gate_attn)

    def visit(blocks, at=slice(None)):
        def stacked(plane):
            parts = [
                kv[b[0], plane, b[1] : b[2]] if isinstance(b, tuple) else kv[b, plane]
                for b in blocks
            ]
            return parts[0] if len(parts) == 1 else jnp.concatenate(parts, axis=0)

        k = stacked(0)
        v = stacked(1)
        scores = [dot(k, q4[i, at, :], 1, 1) for i in range(maps)]
        olds = [m_ref[i, :, at] for i in range(maps)]
        tops = [
            jnp.maximum(old, jnp.max(x, axis=0, keepdims=True)) for old, x in zip(olds, scores)
        ]
        exps = [jnp.exp(x - top) for x, top in zip(scores, tops)]
        factors = [jnp.exp(old - top) for old, top in zip(olds, tops)]
        news = [dot(v, e.astype(BF16), 0, 0) for e in exps]
        for i in range(maps):
            m_ref[i, :, at] = tops[i]
            l_ref[i, :, at] = l_ref[i, :, at] * factors[i] + jnp.sum(exps[i], axis=0, keepdims=True)
            o_ref[i, :, at] = o_ref[i, :, at] * factors[i] + news[i]

    middle = rows // 2

    def mate_arrives(k, halves=(0, 1)):
        for half in halves:
            ref = kv.at[mate - 2 * k, :, half * middle : (half + 1) * middle, :]
            sent(ref, side_recv.at[z - k, half])

    sq_copies = [
        tp_copy(sq_out, sq_in.at[i], sq_send.at[0], sq_recv.at[i], p)
        for i, p in enumerate((p1, p2, p3))
    ]
    high = lax.Precision.HIGHEST

    def convolve():
        @pl.when(s == 0)
        def _():
            gl[:PAD, :] = jnp.zeros((PAD, gl.shape[1]), F32)

        @pl.when(s > 0)
        def _():
            tail.wait_recv()
            gl[:PAD, :] = tail_in[...].astype(F32)

        n_taps = taps_ref.shape[0]
        taps = taps_ref[...].astype(F32)
        conv = jnp.zeros((rows, gl.shape[1]), F32)
        for j in range(n_taps):
            lo = PAD - (n_taps - 1) + j
            conv = conv + gl[lo : lo + rows, :] * taps[j : j + 1, :]
        ones = jnp.ones((8, conv.shape[1]), F32)
        sq_out[...] = dot(ones, conv * conv, 1, 1, high)
        gl[PAD:, :] = conv
        for copy in sq_copies:
            copy.start()
        w_copies[2].start()
    @pl.when(y == 1)
    def _():
        convolve()

    relays(14.01)

    relays(15.25)

    @pl.when(z >= 1)
    def _():
        visit([s - 2])

    relays(15.65)

    @pl.when(y == 0)
    def _():
        convolve()

    relays(16.6)

    @pl.when(y == 1)
    def _():
        mate_arrives(0)

    @pl.when((y == 1) & (z > 0))
    def _():
        visit([mate])

    conv_local = gl.shape[1]
    relays(100.0)

    if last_static >= 2:

        @pl.when(z == 2)
        def _():
            visit([s - 4])

    if last_static >= 3:

        @pl.when(z >= 3)
        def _():
            visit([s - 4, s - 6])

    def beyond(k, carry):
        for q in range(CHUNKS):
            relay(k, q)
        visit([s - 2 * k])
        return carry

    if nz - 1 > NEAR_STEPS:
        lax.fori_loop(NEAR_STEPS + 1, z + 1, beyond, 0)

    conv_local = gl.shape[1]
    gate_conv = projected(5).astype(F32)
    for copy in sq_copies:
        copy.wait_recv()
    total_sq = sq_out[...] + sq_in[0] + sq_in[1] + sq_in[2]
    spread = jnp.full((8, conv_local), 0.125, F32)
    mean_sq = dot(total_sq, spread, 0, 0, high) / (conv_local * n_tp)
    normed = gl[PAD:, :] * lax.rsqrt(mean_sq + EPSILON) * conv_gain[...]
    ybuf[:, :conv_local] = (
        normed * jax.nn.sigmoid(normed) * (gate_conv * jax.nn.sigmoid(gate_conv))
    ).astype(BF16)

    part = rows // n_tp
    both = 2 * part
    far_rows = pl.ds(pl.multiple_of(p2 // 2 * both, both), both)
    near_rows = pl.ds(pl.multiple_of(t // 2 * both, both), both)
    yc_copy = tp_copy(
        ybuf.at[far_rows, :conv_local], yg.at[1, :, :conv_local], g_send.at[1], g_recv.at[1], p3
    )
    ya_copy = tp_copy(
        ybuf.at[far_rows, conv_local:], yg.at[1, :, conv_local:], g_send.at[1], g_recv.at[1], p3
    )
    yc_copy.start()

    def finish(at):
        for h in range(heads):
            first_map = o_ref[2 * h, :, at] / l_ref[2 * h, :, at]
            second_map = o_ref[2 * h + 1, :, at] / l_ref[2 * h + 1, :, at]
            o = first_map - lam[:, h : h + 1] * second_map
            n = o * lax.rsqrt(jnp.mean(o * o, axis=0, keepdims=True) + EPSILON)
            n = jnp.transpose(n) * head_gain[...] * HEAD_SCALE
            lo = h * VDIM
            ybuf[at, conv_local + lo : conv_local + lo + VDIM] = (
                n * ga[at, lo : lo + VDIM]
            ).astype(BF16)

    def beyond_mate(k, carry):
        mate_arrives(k)
        visit([mate - 2 * k])
        return carry

    if nz - 1 > NEAR_STEPS:
        lax.fori_loop(NEAR_STEPS + 1, z + 1, beyond_mate, 0)

    @pl.when(z >= 1)
    def _():
        mate_arrives(1)

    if last_static >= 2:

        @pl.when(z >= 2)
        def _():
            visit([mate - 2])

    if last_static >= 3:

        @pl.when(z >= 3)
        def _():
            mate_arrives(3)
            visit([mate - 6])

    if last_static >= 2:

        @pl.when(z >= 2)
        def _():
            mate_arrives(2, (0,))
            visit([(mate - 4, 0, middle)])
            mate_arrives(2, (1,))

    def last_mate(at):
        @pl.when((z == 0) & (y == 1))
        def _():
            visit([mate], at)

        @pl.when(z == 1)
        def _():
            visit([mate - 2], at)

        if last_static >= 2:

            @pl.when(z >= 2)
            def _():
                visit([(mate - 4, middle, rows)], at)

    last_mate(far_rows)
    finish(far_rows)

    def block(p):
        return ybuf[pl.ds(pl.multiple_of(p * part, part), part), :]

    ya_copy.start()
    lanes = shared // LANES
    edges = [LANES * (lanes * c // PIECES) for c in range(PIECES + 1)]
    ranges = [slice(lo, hi) for lo, hi in zip(edges, edges[1:])]
    far = jnp.concatenate([block(p2), block(p3)], axis=0)
    a_copies = []
    for c, at in enumerate(ranges):
        r = dot(far, w_out[:, at]).astype(BF16)
        a_out[:, at] = r[:part]
        a_own[:, at] = r[part:]
        copy = tp_copy(a_out.at[:, at], a_in.at[:, at], a_sem.at[0], a_sem.at[1 + c], p1)
        copy.start()
        a_copies.append(copy)
    x_copies = []
    for c, at in enumerate(ranges):
        a_copies[c].wait_recv()
        x_out[:, at] = (a_own[:, at].astype(F32) + a_in[:, at].astype(F32)).astype(BF16)
        copy = tp_copy(x_out.at[:, at], x_in.at[:, at], x_sem.at[0], x_sem.at[1 + c], p3)
        copy.start()
        x_copies.append(copy)
    last_mate(near_rows)
    finish(near_rows)
    yn_copy = tp_copy(ybuf.at[near_rows, :], yg.at[0], g_send.at[2], g_recv.at[2], p1)
    yn_copy.start()
    near = jnp.concatenate([block(p1), block(t)], axis=0)
    for c in range(2):
        at = slice(c * (shared // 2), (c + 1) * (shared // 2))
        r = dot(near, w_out[:, at]).astype(BF16)
        b_out[:, at] = r[:part]
        b_own[:, at] = r[part:].astype(F32)
    b_copy = tp_copy(b_out, b_in, b_sem.at[0], b_sem.at[1], p1)
    b_copy.start()
    sent(yg.at[1], g_recv.at[1])
    pass_copy = tp_copy(yg.at[1], yg.at[2], g_send.at[3], g_recv.at[3], p1)
    pass_copy.start()
    sent(wf, g_recv.at[0])
    yn_copy.wait_recv()
    whole = dot(ybuf[near_rows, :], w_out[:, gather_cols(core)])
    whole = whole + dot(yg[0], wf[0]) + dot(yg[1], wf[2])
    pass_copy.wait_recv()
    e_out[...] = (whole + dot(yg[2], wf[1])).astype(BF16)
    e_copy = tp_copy(
        e_out.at[pl.ds(pl.multiple_of((1 - core) * part, part), part)], e_in,
        g_send.at[4], g_recv.at[4], p1,
    )
    e_copy.start()
    sent(tokbuf, tok_send.at[0])
    sent(sq_in, sq_send.at[0])
    sent(a_out, a_sem.at[0])

    @pl.when(s + 1 < n_sp)
    def _():
        tail.wait_send()

    @pl.when(has_up)
    def _():
        sent(kv.at[s], up_send.at[z])

    @pl.when(has_skip)
    def _():
        sent(kv.at[s], skip_send.at[0])

    @pl.when(y == 0)
    def _():
        sent(kv.at[s], side_send.at[z])

    def drain(k, carry):
        j = s - 2 * k

        @pl.when(has_up & (k != SKIP - 1))
        def _():
            sent(kv.at[j], up_send.at[z - k])

        sent(kv.at[j], side_send.at[z - k])
        return carry

    lax.fori_loop(1, z + 1, drain, 0)
    b_copy.wait_recv()
    b_own[...] = b_own[...] + b_in[...].astype(F32)
    e_copy.wait_recv()
    out[:, gather_cols(core)] = e_out[pl.ds(pl.multiple_of(core * part, part), part), :]
    out[:, gather_cols(1 - core)] = e_in[...]
    sent(wf, g_send.at[0])
    sent(yg.at[1], g_send.at[1])
    for copy in (yn_copy, pass_copy, e_copy):
        copy.wait_send()
    for c, at in enumerate(ranges):
        x_copies[c].wait_recv()
        out[:, at] = (b_own[:, at] + x_in[:, at].astype(F32)).astype(BF16)
    sent(x_out, x_sem.at[0])
    sent(b_out, b_sem.at[0])


def local(n_sp, n_tp, *args):
    (tokens, in_gain, w_glu_value, w_glu_gate, w_query, w_key, w_value, w_gate_conv,
     w_gate_attn, conv_weight, conv_gain, lam, head_gain, out_conv, out_attn) = args
    rows, depth = tokens.shape
    width = depth * n_tp
    weights = (w_glu_value, w_glu_gate, w_query, w_key, w_value, w_gate_conv, w_gate_attn)
    total_cols = sum(w.shape[1] for w in weights)
    out_rows = out_conv.shape[0] + out_attn.shape[0]
    out_cols = out_conv.shape[1]
    conv_local = conv_weight.shape[1]
    heads = lam.shape[0]
    part = rows // n_tp
    vmem = pl.BlockSpec(memory_space=pltpu.VMEM)
    hbm = pl.BlockSpec(memory_space=pl.ANY)
    dma = pltpu.SemaphoreType.DMA
    shared = out_cols - 2 * GATHER
    piece = pltpu.VMEM((part, shared), BF16)
    return pl.pallas_call(
        functools.partial(kernel, n_sp, n_tp),
        out_shape=pltpu.VMEM((part, out_cols), BF16),
        in_specs=[hbm] * len(args),
        out_specs=vmem,
        scratch_shapes=[
            pltpu.VMEM((width, total_cols), BF16),
            pltpu.VMEM((out_rows, out_cols), BF16),
            pltpu.VMEM((3, rows, depth), BF16),
            pltpu.VMEM((2, rows, depth), BF16),
            pltpu.VMEM((rows, total_cols), F32),
            pltpu.VMEM((n_sp, 2, rows, VDIM), BF16),
            pltpu.VMEM((2 * heads, rows, 2 * QK), BF16),
            pltpu.VMEM((2 * heads, 1, rows), F32),
            pltpu.VMEM((2 * heads, 1, rows), F32),
            pltpu.VMEM((2 * heads, VDIM, rows), F32),
            pltpu.VMEM((PAD + rows, conv_local), F32),
            pltpu.VMEM((PAD, conv_local), BF16),
            pltpu.VMEM((PAD, conv_local), BF16),
            pltpu.VMEM((8, rows), F32),
            pltpu.VMEM((3, 8, rows), F32),
            pltpu.VMEM((rows, out_rows), BF16),
            piece, piece, piece, piece, piece, piece,
            pltpu.VMEM((part, shared), F32),
            piece,
            pltpu.VMEM((3, out_rows, GATHER), BF16),
            pltpu.VMEM((3, 2 * part, out_rows), BF16),
            pltpu.VMEM((2 * part, GATHER), BF16),
            pltpu.VMEM((part, GATHER), BF16),
            dma((2,)),
            dma((1,)),
            dma((2 * CHUNKS + 1,)),
            dma((max(n_sp // 2 - 1, 1), CHUNKS)),
            dma((n_sp // 2, 2)),
            dma((n_sp // 2,)),
            dma((1,)),
            dma((n_sp // 2,)),
            dma((2,)),
            dma((1,)),
            dma((3,)),
            dma((1 + PIECES,)),
            dma((1 + PIECES,)),
            dma((2,)),
            dma((5,)),
            dma((5,)),
            pltpu.VMEM((width // LANES, LANES), F32),
            pltpu.VMEM(tokens.shape, BF16),
            pltpu.VMEM((width // LANES, LANES), BF16),
            pltpu.VMEM(conv_weight.shape, BF16),
            pltpu.VMEM((1, conv_local), F32),
            pltpu.VMEM((1, heads), F32),
            pltpu.VMEM((1, VDIM), F32),
            pltpu.VMEM((rows, heads * VDIM), F32),
            dma((6,)),
            pltpu.SemaphoreType.REGULAR,
            pltpu.SemaphoreType.REGULAR,
        ],
        compiler_params=pltpu.CompilerParams(
            collective_id=0, has_side_effects=True, vmem_limit_bytes=60 * 1024 * 1024
        ),
    )(
        tokens, in_gain.reshape(width // LANES, LANES), w_glu_value, w_glu_gate, w_query, w_key, w_value,
        w_gate_conv, w_gate_attn, conv_weight, conv_gain.reshape(1, conv_local),
        lam.reshape(1, heads),
        head_gain.reshape(1, VDIM), out_conv, out_attn,
    )


def solution(mesh):
    n_sp, n_tp = mesh.shape["sp"], mesh.shape["tp"]
    assert n_tp == 4 and n_sp % 2 == 0 and 2 * QK == VDIM
    col = P(None, "tp")
    in_specs = (
        P("sp", "tp"), P(), col, col, col, col, col, col, col, col,
        P("tp"), P("tp"), P(), P("tp", None), P("tp", None),
    )
    return jax.shard_map(
        functools.partial(local, n_sp, n_tp), mesh=mesh, in_specs=in_specs,
        out_specs=P(("sp", "tp"), None), check_vma=False,
    )
```
